256 devices in a mesh: kv: 32 (over z, x), tp: 8 (over y, core).
Axes of the slice: x: 4, y: 4, z: 8, core: 2. Of those that a mesh axis runs over, the one named last changes fastest.
Arguments:
- tokens: bfloat16 [1024, 2048], P('kv', 'tp'), may hold values from -60 to 60, as said below
- memory: float32 [1024, 8, 128, 128], P('kv', 'tp'), may hold values from -0.6 to 0.6
- normalizer: float32 [1024, 8, 128], P('kv', 'tp'), may hold values from -0.6 to 0.6
- stabilizer: float32 [1024, 8], P('kv', 'tp'), may hold values from -4 to 4
- norm_gain: float32 [2048], replicated, may hold values from 0.1 to 1.9
- query_weight: bfloat16 [2048, 1024], P(None, 'tp'), may hold values from -0.125 to 0.125
- key_weight: bfloat16 [2048, 1024], P(None, 'tp'), may hold values from -0.125 to 0.125
- value_weight: bfloat16 [2048, 1024], P(None, 'tp'), may hold values from -0.125 to 0.125
- outgate_weight: bfloat16 [2048, 1024], P(None, 'tp'), may hold values from -0.125 to 0.125
- input_gate_weight: bfloat16 [2048, 8], replicated, may hold values from -0.125 to 0.125
- forget_gate_weight: bfloat16 [2048, 8], replicated, may hold values from -0.125 to 0.125
- forget_bias: float32 [8], replicated, may hold values from -1 to 5
- memory_gain: float32 [1024], P('tp'), may hold values from 0.1 to 1.9
- proj_weight: bfloat16 [1024, 2048], P(None, 'tp'), may hold values from -0.1875 to 0.1875
- ffn_gain: float32 [2048], P('tp'), may hold values from 0.1 to 1.9
- up_weight: bfloat16 [2048, 8192], P('tp', 'kv'), may hold values from -0.125 to 0.125
- down_weight: bfloat16 [8192, 2048], P('kv', 'tp'), may hold values from -0.0625 to 0.0625
Outputs:
- layer_out: bfloat16 [1024, 2048], P('kv', 'tp')
- memory_new: float32 [1024, 8, 128, 128], P('kv', 'tp')
- normalizer_new: float32 [1024, 8, 128], P('kv', 'tp')
- stabilizer_new: float32 [1024, 8], P('kv', 'tp')
The draws below stay inside these ranges and needn't reach their ends.
Inputs may be any that keep to these rules, and one draw needn't show every extreme that they name: `tokens`: activations whose feature blocks and rows differ in scale.
All inputs are finite; a program needn't handle non-finite values.
Results may differ from the reference program's by a relative error of at most 0.0095.
Values may be sent and summed in bfloat16 or wider, within the bound.
A program may use at most 64 MiB of HBM per device.

```python
import math
import jax
import jax.numpy as jnp
from jax import lax

D = 2048
H = 8
DK = 128
DV = 128
FF = 8192
SEQS = 1024


def draw_tokens(key, part):
    key_base = jax.random.fold_in(key, 11)
    key_cols = jax.random.fold_in(key, 12)
    key_rows = jax.random.fold_in(key, 13)
    column = jnp.arange(D, dtype=jnp.float32) / (D - 1)
    col_scale = jnp.exp(column * math.log(3.0)) / 1.7 * jnp.exp(jax.random.uniform(key_cols, (D,), jnp.float32, math.log(0.6), math.log(1.6)))
    base = jnp.clip(jax.random.normal(key_base, (SEQS, D), jnp.float32), -4.0, 4.0)
    row_scale = jnp.exp(jax.random.uniform(key_rows, (SEQS, 1), jnp.float32, math.log(0.3), math.log(3.0)))
    return (base * row_scale * col_scale[None, :]).astype(jnp.bfloat16)


def shard_levels(own_key, extent, pieces, low, largest):
    factor_of = 1.0
    for position, blocks in pieces:
        steps = jax.random.uniform(jax.random.fold_in(jax.random.fold_in(own_key, 6), position), (blocks,), jnp.float32, low / len(pieces), largest / len(pieces))
        factor_of = factor_of * jnp.repeat(jnp.exp(steps), extent[position] // blocks).reshape((-1,) + (1,) * (len(extent) - 1 - position))
    return factor_of


def scatter_about(key, extent, width, most, shards=(), kind=jnp.bfloat16):
    values = width * jax.random.normal(key, extent, jnp.float32)
    if shards:
        values = values * shard_levels(key, extent, shards, -0.22, 0.18)
    return jnp.clip(values, -most, most).astype(kind)


def setup_inputs(seed: int = 0) -> dict:
    key_list = jax.random.split(jax.random.key(seed), 18)
    return {
        "tokens": draw_tokens(jax.random.fold_in(key_list[17], 71), 0),
        "memory": scatter_about(key_list[1], (SEQS, H, DV, DK), 0.1, 0.6, ((0, 32), (1, 8)), jnp.float32),
        "normalizer": scatter_about(key_list[2], (SEQS, H, DK), 0.1, 0.6, ((0, 32), (1, 8)), jnp.float32),
        "stabilizer": scatter_about(key_list[3], (SEQS, H), 1.0, 4.0, ((0, 32), (1, 8)), jnp.float32),
        "norm_gain": jnp.clip(1.0 + 0.18 * jax.random.normal(key_list[4], (D,), jnp.float32), 0.1, 1.9),
        "query_weight": scatter_about(key_list[5], (D, H * DK), D ** -0.5, 0.125, ((1, 8),)),
        "key_weight": scatter_about(key_list[6], (D, H * DK), D ** -0.5, 0.125, ((1, 8),)),
        "value_weight": scatter_about(key_list[7], (D, H * DV), D ** -0.5, 0.125, ((1, 8),)),
        "outgate_weight": scatter_about(key_list[8], (D, H * DV), D ** -0.5, 0.125, ((1, 8),)),
        "input_gate_weight": scatter_about(key_list[9], (D, H), D ** -0.5, 0.125),
        "forget_gate_weight": scatter_about(key_list[10], (D, H), D ** -0.5, 0.125),
        "forget_bias": jnp.clip(jax.random.uniform(key_list[11], (H,), jnp.float32, -1.0, 5.0), -1.0, 5.0),
        "memory_gain": jnp.clip(1.0 + 0.18 * jax.random.normal(key_list[12], (H * DV,), jnp.float32), 0.1, 1.9),
        "proj_weight": scatter_about(key_list[13], (H * DV, D), (H * DV) ** -0.5, 0.1875, ((1, 8),)),
        "ffn_gain": jnp.clip(1.0 + 0.18 * jax.random.normal(key_list[14], (D,), jnp.float32), 0.1, 1.9),
        "up_weight": scatter_about(key_list[15], (D, FF), D ** -0.5, 0.125, ((0, 8), (1, 32))),
        "down_weight": scatter_about(key_list[16], (FF, D), FF ** -0.5, 0.0625, ((0, 32), (1, 8))),
    }


EPS = 1e-06

def reference(tokens, memory, normalizer, stabilizer, norm_gain, query_weight, key_weight, value_weight, outgate_weight, input_gate_weight, forget_gate_weight, forget_bias, memory_gain, proj_weight, ffn_gain, up_weight, down_weight):
    rows_f = tokens.astype(jnp.float32)
    scale_one = lax.rsqrt(lax.optimization_barrier(jnp.mean(rows_f * rows_f, axis=-1, keepdims=True)) + EPS)
    normed = (rows_f * scale_one * norm_gain).astype(jnp.bfloat16)
    count = tokens.shape[0]
    query = jnp.dot(normed, query_weight, preferred_element_type=jnp.float32).astype(jnp.bfloat16)
    keys = jnp.dot(normed, key_weight, preferred_element_type=jnp.float32).astype(jnp.bfloat16)
    values = jnp.dot(normed, value_weight, preferred_element_type=jnp.float32).astype(jnp.bfloat16)
    gate_out = jnp.dot(normed, outgate_weight, preferred_element_type=jnp.float32).astype(jnp.bfloat16)
    input_log = jnp.dot(normed, input_gate_weight, preferred_element_type=jnp.float32)
    forget_log = jax.nn.log_sigmoid(jnp.dot(normed, forget_gate_weight, preferred_element_type=jnp.float32) + forget_bias)
    query_f = query.astype(jnp.float32).reshape(count, H, DK)
    keys_f = keys.astype(jnp.float32).reshape(count, H, DK) * DK ** (-0.5)
    values_f = values.astype(jnp.float32).reshape(count, H, DV)
    stab_new = jnp.maximum(forget_log + stabilizer, input_log)
    keep = jnp.exp(forget_log + stabilizer - stab_new)
    admit = jnp.exp(input_log - stab_new)
    memory_new = keep[..., None, None] * memory + admit[..., None, None] * values_f[..., :, None] * keys_f[..., None, :]
    normalizer_new = keep[..., None] * normalizer + admit[..., None] * keys_f
    numer = jnp.einsum('bhed,bhd->bhe', memory_new, query_f, precision=lax.Precision.HIGHEST)
    denom = lax.optimization_barrier(jnp.sum(normalizer_new * query_f, axis=-1))
    cell = numer / jnp.maximum(jnp.abs(denom), 1.0)[..., None]
    mixed = (cell.reshape(count, H * DV) * memory_gain * jax.nn.sigmoid(gate_out.astype(jnp.float32))).astype(jnp.bfloat16)
    second = (rows_f + jnp.dot(mixed, proj_weight, preferred_element_type=jnp.float32)).astype(jnp.bfloat16)
    second_f = second.astype(jnp.float32)
    scale_two = lax.rsqrt(lax.optimization_barrier(jnp.mean(second_f * second_f, axis=-1, keepdims=True)) + EPS)
    scaled = (second_f * ffn_gain).astype(jnp.bfloat16)
    preact = jnp.dot(scaled, up_weight, preferred_element_type=jnp.float32)
    hidden = jnp.square(jax.nn.relu(preact * scale_two)).astype(jnp.bfloat16)
    layer_out = (second_f + jnp.dot(hidden, down_weight, preferred_element_type=jnp.float32)).astype(jnp.bfloat16)
    return (layer_out, memory_new, normalizer_new, stab_new)
```

```python
import jax
import jax.numpy as jnp
from jax import lax
from jax.experimental import pallas as pl
from jax.experimental.pallas import tpu as pltpu
from jax.sharding import PartitionSpec as P

D = 2048
DK = 128
EPS = 1e-06
XN = 4
ZN = 8
YN = 4
TN = 8
ROWS = 32
DB = D // TN
SUB = ROWS // TN
FB = 256
ZORD = (0, 1, 7, 2, 6, 3, 5, 4)
ZPOS = tuple(ZORD.index(o) for o in range(ZN))
TPO = ((2, 0), (2, 1), (1, 0), (1, 1), (3, 0), (3, 1), (0, 1))
GROUPS = ZN // 2
F32 = jnp.float32
BF16 = jnp.bfloat16
MESH = pl.DeviceIdType.MESH


def remote(src, dst, send_sem, recv_sem, kv, tp):
    return pltpu.make_async_remote_copy(
        src_ref=src,
        dst_ref=dst,
        send_sem=send_sem,
        recv_sem=recv_sem,
        device_id={"kv": kv, "tp": tp},
        device_id_type=MESH,
    )


def await_bytes(ref, sem):
    pltpu.make_async_copy(ref, ref, sem).wait()


def kernel(
    tok_h, mem_h, nrm_h, stab_h, ng_h, qw_h, kw_h, vw_h, ow_h, ig_h, fg_h, fb_h, mg_h, pw_h, gain_h, up_h, dn_h,
    out_ref, memn_h, nrmn_ref, stabn_ref,
    tk, mem, nrm, stab, ng, qkvo, ig, fg, fb, mg, pw, gains, upb, dnb,
    nb, qf, colrow, colmat, mx, secf, seg, xbuf, xs, os, rsx_s, rsx_r, own, zs, fin, of,
    lsem, tok_s, tok_r, gain_s, gain_r, mix_s, mix_r, w_s, w_r, az_s, az_r, xf_s, xf_r, rx_s, rx_r, fi_s, fi_r,
    zready,
):
    kv = lax.axis_index("kv")
    t = lax.axis_index("tp")
    z, x = kv // XN, kv % XN
    y, c = t // 2, t % 2

    def zx(dz, dx):
        return ((z + dz) % ZN) * XN + (x + dx) % XN

    def tp_at(dy, dc):
        return ((y + dy) % YN) * 2 + (c + dc) % 2

    pending = []

    def send(src, dst, ssem, rsem, kv_to, tp_to):
        remote(src, dst, ssem, rsem, kv_to, tp_to).start()
        pending.append((src, ssem))

    lane_t = pl.ds(pl.multiple_of(t * DB, DB), DB)
    lane_h = pl.ds(pl.multiple_of(t * DK, DK), DK)
    row_t = lane_t

    loads = {}

    def load(name, src, dst):
        k = len(loads)
        loads[name] = pltpu.make_async_copy(src, dst, lsem.at[k])
        loads[name].start()

    load("tok", tok_h, tk.at[:, lane_t])
    load("gain", gain_h, gains.at[:, lane_t])
    load("up", up_h, upb.at[row_t])
    load("dn", dn_h, dnb.at[t])
    load("ng", ng_h, ng)
    for k, (name, w) in enumerate((("q", qw_h), ("k", kw_h), ("v", vw_h), ("o", ow_h))):
        load(name, w, qkvo.at[:, DK * k : DK * (k + 1)])
    load("ig", ig_h, ig)
    load("fg", fg_h, fg)
    load("fb", fb_h, fb)
    load("stab", stab_h, stab)
    load("nrm", nrm_h, nrm)
    load("mem", mem_h, mem)
    load("mg", mg_h, mg)
    load("pw", pw_h, pw)

    barrier = pltpu.get_barrier_semaphore()
    for dy, dc in TPO:
        pl.semaphore_signal(barrier, inc=1, device_id={"kv": kv, "tp": tp_at(dy, dc)}, device_id_type=MESH)
    for dx in range(1, XN):
        pl.semaphore_signal(barrier, inc=1, device_id={"kv": zx(0, dx), "tp": t}, device_id_type=MESH)
    for dz in range(1, ZN):
        pl.semaphore_signal(barrier, inc=1, device_id={"kv": zx(dz, 0), "tp": t}, device_id_type=MESH)
    pl.semaphore_wait(barrier, 7 + (XN - 1) + (ZN - 1))
    for dz in range(1, ZN):
        pl.semaphore_signal(zready, inc=1, device_id={"kv": zx(dz, 0), "tp": t}, device_id_type=MESH)

    loads["tok"].wait()
    for k, (dy, dc) in enumerate(TPO):
        send(tk.at[:, lane_t], tk.at[:, lane_t], tok_s.at[k], tok_r.at[k], kv, tp_at(dy, dc))
    loads["gain"].wait()
    for k, (dy, dc) in enumerate(TPO):
        send(gains.at[:, lane_t], gains.at[:, lane_t], gain_s.at[k], gain_r.at[k], kv, tp_at(dy, dc))

    def w_slot(m, dy, dc):
        s = tp_at(dy, dc)
        return upb.at[pl.ds(pl.multiple_of(s * DB, DB), DB)] if m == 0 else dnb.at[s]

    loads["up"].wait()
    send(w_slot(0, 0, 0), w_slot(0, 0, 0), w_s.at[0, 0], w_r.at[0, 0], kv, tp_at(1, 0))
    send(w_slot(0, 0, 0), w_slot(0, 0, 0), w_s.at[0, 1], w_r.at[0, 1], kv, tp_at(3, 0))
    send(w_slot(0, 0, 0), w_slot(0, 0, 0), w_s.at[0, 3], w_r.at[0, 3], kv, tp_at(0, 1))
    loads["dn"].wait()
    send(w_slot(1, 0, 0), w_slot(1, 0, 0), w_s.at[1, 0], w_r.at[1, 0], kv, tp_at(1, 0))
    send(w_slot(1, 0, 0), w_slot(1, 0, 0), w_s.at[1, 1], w_r.at[1, 1], kv, tp_at(3, 0))
    send(w_slot(1, 0, 0), w_slot(1, 0, 0), w_s.at[1, 3], w_r.at[1, 3], kv, tp_at(0, 1))

    for name in ("ng", "q", "k", "v", "o", "ig", "fg", "fb", "stab", "nrm"):
        loads[name].wait()
    for k, (dy, dc) in enumerate(TPO):
        s = tp_at(-dy, -dc)
        await_bytes(tk.at[:, pl.ds(pl.multiple_of(s * DB, DB), DB)], tok_r.at[k])
    rows = tk[...].astype(F32)
    scale_one = lax.rsqrt(jnp.sum(rows * rows, axis=-1, keepdims=True) * (1.0 / D) + EPS)
    nb[...] = (rows * scale_one * ng[...]).astype(BF16)
    proj4 = jnp.dot(nb[...], qkvo[...], preferred_element_type=F32).astype(BF16).astype(F32)
    query = proj4[:, :DK]
    keys = proj4[:, DK : 2 * DK] * DK ** (-0.5)
    values = proj4[:, 2 * DK : 3 * DK]
    gate_out = proj4[:, 3 * DK :]
    qf[...] = query

    contract = (((1,), (1,)), ((), ()))
    all_in = lax.dot_general(nb[...], ig[...], contract, preferred_element_type=F32)
    all_forget = lax.dot_general(nb[...], fg[...], contract, preferred_element_type=F32) + fb[...]
    head = lax.broadcasted_iota(jnp.int32, (ROWS, TN), 1) == t
    input_log = jnp.sum(jnp.where(head, all_in, 0.0), axis=1, keepdims=True)
    raw = jnp.sum(jnp.where(head, all_forget, 0.0), axis=1, keepdims=True)
    forget_log = jnp.minimum(raw, 0.0) - jnp.log1p(jnp.exp(-jnp.abs(raw)))
    diag = lax.broadcasted_iota(jnp.int32, (ROWS, ROWS), 0) == lax.broadcasted_iota(jnp.int32, (ROWS, ROWS), 1)
    stab_col = jnp.sum(jnp.where(diag, jnp.broadcast_to(stab[...], (ROWS, ROWS)), 0.0), axis=1, keepdims=True)
    stab_new = jnp.maximum(forget_log + stab_col, input_log)
    keep = jnp.exp(forget_log + stab_col - stab_new)
    admit = jnp.exp(input_log - stab_new)
    normalizer_new = keep * nrm[...] + admit * keys
    denom = jnp.sum(normalizer_new * query, axis=1, keepdims=True)
    key_query = jnp.sum(keys * query, axis=1, keepdims=True)

    loads["mem"].wait()
    lane = lax.broadcasted_iota(jnp.int32, (DK, DK), 1)

    def read_memory(b, acc):
        part = jnp.sum(mem[b] * qf[pl.ds(b, 1), :], axis=1, keepdims=True)
        return jnp.where(lane == b, part, acc)

    read = lax.fori_loop(0, ROWS, read_memory, jnp.zeros((DK, DK), F32), unroll=4)
    memory_query = read.T[:ROWS, :]
    numer = keep * memory_query + (admit * key_query) * values
    cell = numer / jnp.maximum(jnp.abs(denom), 1.0)
    loads["mg"].wait()
    mx[:, lane_h] = (cell * mg[...] * jax.nn.sigmoid(gate_out)).astype(BF16)
    for k, (dy, dc) in enumerate(TPO):
        send(mx.at[:, lane_h], mx.at[:, lane_h], mix_s.at[k], mix_r.at[k], kv, tp_at(dy, dc))

    nrmn_ref[...] = normalizer_new
    stabn_ref[...] = jnp.sum(
        jnp.where(diag, jnp.broadcast_to(stab_new, (ROWS, ROWS)), 0.0), axis=0, keepdims=True
    )
    colrow[0] = jnp.broadcast_to(keep, (ROWS, DK))
    colrow[1] = keys
    colmat[:ROWS, :] = admit * values
    colmat[ROWS:, :] = jnp.zeros((DK - ROWS, DK), F32)
    admitted = colmat[...].T

    def write_memory(b, carry):
        column = jnp.sum(jnp.where(lane == b, admitted, 0.0), axis=1, keepdims=True)
        mem[b] = colrow[0, pl.ds(b, 1), :] * mem[b] + column * colrow[1, pl.ds(b, 1), :]
        return carry

    lax.fori_loop(0, ROWS, write_memory, 0, unroll=4)
    store_mem = pltpu.make_async_copy(mem, memn_h, lsem.at[len(loads)])
    store_mem.start()

    loads["pw"].wait()
    for k, (dy, dc) in enumerate(TPO):
        s = tp_at(-dy, -dc)
        await_bytes(mx.at[:, pl.ds(pl.multiple_of(s * DK, DK), DK)], mix_r.at[k])
    projected = jnp.dot(mx[...], pw[...], preferred_element_type=F32)
    second = (tk[:, lane_t].astype(F32) + projected).astype(BF16).astype(F32)
    secf[...] = second
    for s in range(TN):
        seg[s] = secf[SUB * s : SUB * (s + 1), :].astype(BF16)

    pl.semaphore_wait(zready, ZN - 1)
    own_seg = pltpu.make_async_copy(seg.at[t], xbuf.at[0, 0, t], az_r.at[0])
    own_seg.start()
    for dz in (4, 3, 5, 2, 6, 1, 7, 0):
        there = ZPOS[(-dz) % ZN]
        for dy, dc in TPO if dz == 0 else TPO + ((0, 0),):
            s = tp_at(dy, dc)
            remote(
                seg.at[s], xbuf.at[0, there, t], az_s.at[ZPOS[dz]], az_r.at[there], zx(dz, 0), s
            ).start()

    def relay(m, k, dy, forward):
        slot = w_slot(m, dy, 0)
        await_bytes(slot, w_r.at[m, k])
        if forward is not None:
            send(slot, slot, w_s.at[m, 2], w_r.at[m, 2], kv, tp_at(forward, 0))
        send(slot, slot, w_s.at[m, 4 + k], w_r.at[m, 4 + k], kv, tp_at(0, 1))

    relay(0, 0, 3, 1)
    relay(1, 1, 1, 3)
    relay(0, 1, 1, None)
    relay(1, 0, 3, None)

    for g in range(GROUPS):
        for p in (2 * g, 2 * g + 1):
            await_bytes(xbuf.at[0, p], az_r.at[p])
        pair = pl.ds(2 * g, 2)
        for dx in range(1, XN):
            send(
                xbuf.at[0, pair], xbuf.at[(-dx) % XN, pair],
                xf_s.at[dx - 1, g], xf_r.at[(-dx) % XN - 1, g], zx(0, dx), t,
            )

    relay(0, 2, 2, None)
    relay(1, 2, 2, None)
    for k, (dy, dc) in enumerate(TPO):
        s = tp_at(-dy, -dc)
        await_bytes(gains.at[:, pl.ds(pl.multiple_of(s * DB, DB), DB)], gain_r.at[k])
    for m in range(2):
        for k, dy in ((3, 0), (4, 3), (5, 1), (6, 2)):
            await_bytes(w_slot(m, dy, 1), w_r.at[m, k])

    def mixer(g):
        for dx in range(1, XN):
            await_bytes(xbuf.at[dx, pl.ds(2 * g, 2)], xf_r.at[dx - 1, g])
        for i in range(2 * XN):
            dx, p = i // 2, 2 * g + i % 2
            block = xbuf[dx, p].astype(F32)
            for j in range(TN):
                xs[SUB * i : SUB * (i + 1), DB * j : DB * (j + 1)] = block[j]
        sec = xs[...]
        scale_two = lax.rsqrt(jnp.sum(sec * sec, axis=-1, keepdims=True) * (1.0 / D) + EPS)
        scaled = (sec * gains[...]).astype(BF16)
        preact = jnp.dot(scaled, upb[...], preferred_element_type=F32)
        hidden = jnp.square(jnp.maximum(preact * scale_two, 0.0)).astype(BF16)
        for j in range(TN):
            os[:, DB * j : DB * (j + 1)] = jnp.dot(hidden, dnb[j], preferred_element_type=F32)
        for i in range(2 * XN):
            dx, p = i // 2, 2 * g + i % 2
            for j in range(TN):
                block = os[SUB * i : SUB * (i + 1), DB * j : DB * (j + 1)]
                if dx == 0:
                    own[p, j] = block
                else:
                    rsx_s[dx - 1, p, j] = block.astype(BF16)
        pair = pl.ds(2 * g, 2)
        for dx in range(1, XN):
            send(
                rsx_s.at[dx - 1, pair], rsx_r.at[(-dx) % XN - 1, pair],
                rx_s.at[dx - 1, g], rx_r.at[(-dx) % XN - 1, g], zx(0, dx), t,
            )

    def sum_x(g):
        pair = pl.ds(2 * g, 2)
        for dx in range(1, XN):
            await_bytes(rsx_r.at[dx - 1, pair], rx_r.at[dx - 1, g])
        for p in (2 * g, 2 * g + 1):
            total = own[p]
            for dx in range(1, XN):
                total += rsx_r[dx - 1, p].astype(F32)
            zs[p] = total.astype(BF16)
            dz = ZORD[p]
            there = ZPOS[(-dz) % ZN]
            if dz == 0:
                pltpu.make_async_copy(zs.at[p, t], fin.at[0, t], fi_r.at[0]).start()
            for dy, dc in TPO if dz == 0 else TPO + ((0, 0),):
                s = tp_at(dy, dc)
                remote(
                    zs.at[p, s], fin.at[there, t], fi_s.at[p], fi_r.at[there], zx(dz, 0), s
                ).start()

    mixer(0)
    for g in range(1, GROUPS):
        mixer(g)
        sum_x(g - 1)
    sum_x(GROUPS - 1)

    total = jnp.zeros((TN, SUB, DB), F32)
    for p in range(ZN):
        await_bytes(fin.at[p], fi_r.at[p])
        total += fin[p].astype(F32)
    for s in range(TN):
        of[SUB * s : SUB * (s + 1), :] = total[s]
    out_ref[...] = (secf[...] + of[...]).astype(BF16)

    for src, sem in pending:
        await_bytes(src, sem)
    for p in range(ZN):
        count = TN - 1 if p == 0 else TN
        await_bytes(seg.at[pl.ds(0, count)], az_s.at[p])
        await_bytes(zs.at[p, pl.ds(0, count)], fi_s.at[p])
    store_mem.wait()


def per_device(
    tokens, memory, normalizer, stabilizer, norm_gain, query_weight, key_weight, value_weight, outgate_weight,
    input_gate_weight, forget_gate_weight, forget_bias, memory_gain, proj_weight, ffn_gain, up_weight, down_weight,
):
    hbm = pl.BlockSpec(memory_space=pl.ANY)
    vmem = pl.BlockSpec(memory_space=pltpu.VMEM)
    dma = pltpu.SemaphoreType.DMA
    layer_out, memory_new, normalizer_new, stab_new = pl.pallas_call(
        kernel,
        out_shape=(
            jax.ShapeDtypeStruct((ROWS, DB), BF16),
            jax.ShapeDtypeStruct((ROWS, DK, DK), F32),
            jax.ShapeDtypeStruct((ROWS, DK), F32),
            jax.ShapeDtypeStruct((1, ROWS), F32),
        ),
        in_specs=[hbm] * 17,
        out_specs=(vmem, hbm, vmem, vmem),
        scratch_shapes=[
            pltpu.VMEM((ROWS, D), BF16),
            pltpu.VMEM((ROWS, DK, DK), F32),
            pltpu.VMEM((ROWS, DK), F32),
            pltpu.VMEM((1, ROWS), F32),
            pltpu.VMEM((1, D), F32),
            pltpu.VMEM((D, 4 * DK), BF16),
            pltpu.VMEM((TN, D), BF16),
            pltpu.VMEM((TN, D), BF16),
            pltpu.VMEM((1, TN), F32),
            pltpu.VMEM((1, DK), F32),
            pltpu.VMEM((TN * DK, DB), BF16),
            pltpu.VMEM((1, D), F32),
            pltpu.VMEM((D, FB), BF16),
            pltpu.VMEM((TN, FB, DB), BF16),
            pltpu.VMEM((ROWS, D), BF16),
            pltpu.VMEM((ROWS, DK), F32),
            pltpu.VMEM((2, ROWS, DK), F32),
            pltpu.VMEM((DK, DK), F32),
            pltpu.VMEM((ROWS, TN * DK), BF16),
            pltpu.VMEM((ROWS, DB), F32),
            pltpu.VMEM((TN, SUB, DB), BF16),
            pltpu.VMEM((XN, ZN, TN, SUB, DB), BF16),
            pltpu.VMEM((ROWS, D), F32),
            pltpu.VMEM((ROWS, D), F32),
            pltpu.VMEM((XN - 1, ZN, TN, SUB, DB), BF16),
            pltpu.VMEM((XN - 1, ZN, TN, SUB, DB), BF16),
            pltpu.VMEM((ZN, TN, SUB, DB), F32),
            pltpu.VMEM((ZN, TN, SUB, DB), BF16),
            pltpu.VMEM((ZN, TN, SUB, DB), BF16),
            pltpu.VMEM((ROWS, DB), F32),
            dma((18,)),
            dma((7,)), dma((7,)),
            dma((7,)), dma((7,)),
            dma((7,)), dma((7,)),
            dma((2, 7)), dma((2, 7)),
            dma((ZN,)), dma((ZN,)),
            dma((XN - 1, GROUPS)), dma((XN - 1, GROUPS)),
            dma((XN - 1, GROUPS)), dma((XN - 1, GROUPS)),
            dma((ZN,)), dma((ZN,)),
            pltpu.SemaphoreType.REGULAR,
        ],
        compiler_params=pltpu.CompilerParams(
            collective_id=0, has_side_effects=True, vmem_limit_bytes=40 * 1024 * 1024
        ),
        name="layer",
    )(
        tokens,
        memory.reshape(ROWS, DK, DK),
        normalizer.reshape(ROWS, DK),
        stabilizer.T,
        norm_gain.reshape(1, D),
        query_weight, key_weight, value_weight, outgate_weight,
        input_gate_weight.T,
        forget_gate_weight.T,
        forget_bias.reshape(1, TN),
        memory_gain.reshape(1, DK),
        proj_weight,
        ffn_gain.reshape(1, DB),
        up_weight,
        down_weight,
    )
    return (
        layer_out,
        memory_new.reshape(ROWS, 1, DK, DK),
        normalizer_new.reshape(ROWS, 1, DK),
        stab_new.T,
    )


def solution(mesh):
    placed = (
        P("kv", "tp"),
        P("kv", "tp", None, None),
        P("kv", "tp", None),
        P("kv", "tp"),
        P(),
        P(None, "tp"),
        P(None, "tp"),
        P(None, "tp"),
        P(None, "tp"),
        P(),
        P(),
        P(),
        P("tp"),
        P(None, "tp"),
        P("tp"),
        P("tp", "kv"),
        P("kv", "tp"),
    )
    outs = (P("kv", "tp"), P("kv", "tp", None, None), P("kv", "tp", None), P("kv", "tp"))
    return jax.shard_map(per_device, mesh=mesh, in_specs=placed, out_specs=outs, check_vma=False)
```

```python
import jax
import jax.numpy as jnp
from jax import lax
from jax.experimental import pallas as pl
from jax.experimental.pallas import tpu as pltpu
from jax.sharding import PartitionSpec as P

D = 2048
DK = 128
EPS = 1e-06
XN = 4
ZN = 8
YN = 4
TN = 8
ROWS = 32
DB = D // TN
SUB = ROWS // TN
FB = 256
ZORD = (0, 1, 7, 2, 6, 3, 5, 4)
ZPOS = tuple(ZORD.index(o) for o in range(ZN))
TPO = ((2, 0), (2, 1), (1, 0), (1, 1), (3, 0), (3, 1), (0, 1))
GROUPS = ZN // 2
F32 = jnp.float32
BF16 = jnp.bfloat16
MESH = pl.DeviceIdType.MESH


def remote(src, dst, send_sem, recv_sem, kv, tp):
    return pltpu.make_async_remote_copy(
        src_ref=src,
        dst_ref=dst,
        send_sem=send_sem,
        recv_sem=recv_sem,
        device_id={"kv": kv, "tp": tp},
        device_id_type=MESH,
    )


def await_bytes(ref, sem):
    pltpu.make_async_copy(ref, ref, sem).wait()


def kernel(
    tok_h, mem_h, nrm_h, stab_h, ng_h, qw_h, kw_h, vw_h, ow_h, ig_h, fg_h, fb_h, mg_h, pw_h, gain_h, up_h, dn_h,
    out_ref, memn_h, nrmn_ref, stabn_ref,
    tk, mem, nrm, stab, ng, qkvo, ig, fg, fb, mg, pw, gains, upb, dnb,
    nb, qf, colrow, colmat, mx, secf, seg, xbuf, xs, os, rsx_s, rsx_r, own, zs, fin, of,
    lsem, tok_s, tok_r, gain_s, gain_r, mix_s, mix_r, w_s, w_r, az_s, az_r, xf_s, xf_r, rx_s, rx_r, fi_s, fi_r,
    zready,
):
    kv = lax.axis_index("kv")
    t = lax.axis_index("tp")
    z, x = kv // XN, kv % XN
    y, c = t // 2, t % 2

    def zx(dz, dx):
        return ((z + dz) % ZN) * XN + (x + dx) % XN

    def tp_at(dy, dc):
        return ((y + dy) % YN) * 2 + (c + dc) % 2

    pending = []

    def send(src, dst, ssem, rsem, kv_to, tp_to):
        remote(src, dst, ssem, rsem, kv_to, tp_to).start()
        pending.append((src, ssem))

    lane_t = pl.ds(pl.multiple_of(t * DB, DB), DB)
    lane_h = pl.ds(pl.multiple_of(t * DK, DK), DK)
    row_t = lane_t

    loads = {}

    def load(name, src, dst):
        k = len(loads)
        loads[name] = pltpu.make_async_copy(src, dst, lsem.at[k])
        loads[name].start()

    load("tok", tok_h, tk.at[:, lane_t])
    load("gain", gain_h, gains.at[:, lane_t])
    load("up", up_h, upb.at[row_t])
    load("dn", dn_h, dnb.at[t])
    load("ng", ng_h, ng)
    for k, (name, w) in enumerate((("q", qw_h), ("k", kw_h), ("v", vw_h), ("o", ow_h))):
        load(name, w, qkvo.at[:, DK * k : DK * (k + 1)])
    load("ig", ig_h, ig)
    load("fg", fg_h, fg)
    load("fb", fb_h, fb)
    load("stab", stab_h, stab)
    load("nrm", nrm_h, nrm)
    load("mem", mem_h, mem)
    load("mg", mg_h, mg)
    load("pw", pw_h, pw)

    barrier = pltpu.get_barrier_semaphore()
    for dy, dc in TPO:
        pl.semaphore_signal(barrier, inc=1, device_id={"kv": kv, "tp": tp_at(dy, dc)}, device_id_type=MESH)
    for dx in range(1, XN):
        pl.semaphore_signal(barrier, inc=1, device_id={"kv": zx(0, dx), "tp": t}, device_id_type=MESH)
    for dz in range(1, ZN):
        pl.semaphore_signal(barrier, inc=1, device_id={"kv": zx(dz, 0), "tp": t}, device_id_type=MESH)
    pl.semaphore_wait(barrier, 7 + (XN - 1) + (ZN - 1))
    for dz in range(1, ZN):
        pl.semaphore_signal(zready, inc=1, device_id={"kv": zx(dz, 0), "tp": t}, device_id_type=MESH)

    loads["tok"].wait()
    for k, (dy, dc) in enumerate(TPO):
        send(tk.at[:, lane_t], tk.at[:, lane_t], tok_s.at[k], tok_r.at[k], kv, tp_at(dy, dc))
    loads["gain"].wait()
    for k, (dy, dc) in enumerate(TPO):
        send(gains.at[:, lane_t], gains.at[:, lane_t], gain_s.at[k], gain_r.at[k], kv, tp_at(dy, dc))

    def w_slot(m, dy, dc):
        s = tp_at(dy, dc)
        return upb.at[pl.ds(pl.multiple_of(s * DB, DB), DB)] if m == 0 else dnb.at[s]

    loads["up"].wait()
    send(w_slot(0, 0, 0), w_slot(0, 0, 0), w_s.at[0, 0], w_r.at[0, 0], kv, tp_at(1, 0))
    send(w_slot(0, 0, 0), w_slot(0, 0, 0), w_s.at[0, 1], w_r.at[0, 1], kv, tp_at(3, 0))
    send(w_slot(0, 0, 0), w_slot(0, 0, 0), w_s.at[0, 3], w_r.at[0, 3], kv, tp_at(0, 1))
    loads["dn"].wait()
    send(w_slot(1, 0, 0), w_slot(1, 0, 0), w_s.at[1, 0], w_r.at[1, 0], kv, tp_at(1, 0))
    send(w_slot(1, 0, 0), w_slot(1, 0, 0), w_s.at[1, 1], w_r.at[1, 1], kv, tp_at(3, 0))
    send(w_slot(1, 0, 0), w_slot(1, 0, 0), w_s.at[1, 3], w_r.at[1, 3], kv, tp_at(0, 1))

    for name in ("ng", "q", "k", "v", "o", "ig", "fg", "fb", "stab", "nrm"):
        loads[name].wait()
    for k, (dy, dc) in enumerate(TPO):
        s = tp_at(-dy, -dc)
        await_bytes(tk.at[:, pl.ds(pl.multiple_of(s * DB, DB), DB)], tok_r.at[k])
    rows = tk[...].astype(F32)
    scale_one = lax.rsqrt(jnp.sum(rows * rows, axis=-1, keepdims=True) * (1.0 / D) + EPS)
    nb[...] = (rows * scale_one * ng[...]).astype(BF16)
    proj4 = jnp.dot(nb[...], qkvo[...], preferred_element_type=F32).astype(BF16).astype(F32)
    query = proj4[:, :DK]
    keys = proj4[:, DK : 2 * DK] * DK ** (-0.5)
    values = proj4[:, 2 * DK : 3 * DK]
    gate_out = proj4[:, 3 * DK :]
    qf[...] = query

    contract = (((1,), (1,)), ((), ()))
    all_in = lax.dot_general(nb[...], ig[...], contract, preferred_element_type=F32)
    all_forget = lax.dot_general(nb[...], fg[...], contract, preferred_element_type=F32) + fb[...]
    head = lax.broadcasted_iota(jnp.int32, (ROWS, TN), 1) == t
    input_log = jnp.sum(jnp.where(head, all_in, 0.0), axis=1, keepdims=True)
    raw = jnp.sum(jnp.where(head, all_forget, 0.0), axis=1, keepdims=True)
    forget_log = jnp.minimum(raw, 0.0) - jnp.log1p(jnp.exp(-jnp.abs(raw)))
    diag = lax.broadcasted_iota(jnp.int32, (ROWS, ROWS), 0) == lax.broadcasted_iota(jnp.int32, (ROWS, ROWS), 1)
    stab_col = jnp.sum(jnp.where(diag, jnp.broadcast_to(stab[...], (ROWS, ROWS)), 0.0), axis=1, keepdims=True)
    stab_new = jnp.maximum(forget_log + stab_col, input_log)
    keep = jnp.exp(forget_log + stab_col - stab_new)
    admit = jnp.exp(input_log - stab_new)
    normalizer_new = keep * nrm[...] + admit * keys
    denom = jnp.sum(normalizer_new * query, axis=1, keepdims=True)
    key_query = jnp.sum(keys * query, axis=1, keepdims=True)

    loads["mem"].wait()
    lane = lax.broadcasted_iota(jnp.int32, (DK, DK), 1)

    def read_memory(b, acc):
        part = jnp.sum(mem[b] * qf[pl.ds(b, 1), :], axis=1, keepdims=True)
        return jnp.where(lane == b, part, acc)

    read = lax.fori_loop(0, ROWS, read_memory, jnp.zeros((DK, DK), F32), unroll=4)
    memory_query = read.T[:ROWS, :]
    numer = keep * memory_query + (admit * key_query) * values
    cell = numer / jnp.maximum(jnp.abs(denom), 1.0)
    loads["mg"].wait()
    mx[:, lane_h] = (cell * mg[...] * jax.nn.sigmoid(gate_out)).astype(BF16)
    for k, (dy, dc) in enumerate(TPO):
        send(mx.at[:, lane_h], mx.at[:, lane_h], mix_s.at[k], mix_r.at[k], kv, tp_at(dy, dc))

    nrmn_ref[...] = normalizer_new
    stabn_ref[...] = jnp.sum(
        jnp.where(diag, jnp.broadcast_to(stab_new, (ROWS, ROWS)), 0.0), axis=0, keepdims=True
    )
    colrow[0] = jnp.broadcast_to(keep, (ROWS, DK))
    colrow[1] = keys
    colmat[:ROWS, :] = admit * values
    colmat[ROWS:, :] = jnp.zeros((DK - ROWS, DK), F32)
    admitted = colmat[...].T

    def write_memory(b, carry):
        column = jnp.sum(jnp.where(lane == b, admitted, 0.0), axis=1, keepdims=True)
        mem[b] = colrow[0, pl.ds(b, 1), :] * mem[b] + column * colrow[1, pl.ds(b, 1), :]
        return carry

    lax.fori_loop(0, ROWS, write_memory, 0, unroll=4)
    store_mem = pltpu.make_async_copy(mem, memn_h, lsem.at[len(loads)])
    store_mem.start()

    loads["pw"].wait()
    for k, (dy, dc) in enumerate(TPO):
        s = tp_at(-dy, -dc)
        await_bytes(mx.at[:, pl.ds(pl.multiple_of(s * DK, DK), DK)], mix_r.at[k])
    projected = jnp.dot(mx[...], pw[...], preferred_element_type=F32)
    second = (tk[:, lane_t].astype(F32) + projected).astype(BF16).astype(F32)
    secf[...] = second
    for s in range(TN):
        seg[s] = secf[SUB * s : SUB * (s + 1), :].astype(BF16)

    pl.semaphore_wait(zready, ZN - 1)
    own_seg = pltpu.make_async_copy(seg.at[t], xbuf.at[0, 0, t], az_r.at[0])
    own_seg.start()
    for dz in (4, 3, 5, 2, 6, 1, 7, 0):
        there = ZPOS[(-dz) % ZN]
        for dy, dc in TPO if dz == 0 else TPO + ((0, 0),):
            s = tp_at(dy, dc)
            remote(
                seg.at[s], xbuf.at[0, there, t], az_s.at[ZPOS[dz]], az_r.at[there], zx(dz, 0), s
            ).start()

    def relay(m, k, dy, forward):
        slot = w_slot(m, dy, 0)
        await_bytes(slot, w_r.at[m, k])
        if forward is not None:
            send(slot, slot, w_s.at[m, 2], w_r.at[m, 2], kv, tp_at(forward, 0))
        send(slot, slot, w_s.at[m, 4 + k], w_r.at[m, 4 + k], kv, tp_at(0, 1))

    relay(0, 0, 3, 1)
    relay(1, 1, 1, 3)
    relay(0, 1, 1, None)
    relay(1, 0, 3, None)

    for g in range(GROUPS):
        for p in (2 * g, 2 * g + 1):
            await_bytes(xbuf.at[0, p], az_r.at[p])
        pair = pl.ds(2 * g, 2)
        for dx in range(1, XN):
            send(
                xbuf.at[0, pair], xbuf.at[(-dx) % XN, pair],
                xf_s.at[dx - 1, g], xf_r.at[(-dx) % XN - 1, g], zx(0, dx), t,
            )

    relay(0, 2, 2, None)
    relay(1, 2, 2, None)
    for k, (dy, dc) in enumerate(TPO):
        s = tp_at(-dy, -dc)
        await_bytes(gains.at[:, pl.ds(pl.multiple_of(s * DB, DB), DB)], gain_r.at[k])
    for m in range(2):
        for k, dy in ((3, 0), (4, 3), (5, 1), (6, 2)):
            await_bytes(w_slot(m, dy, 1), w_r.at[m, k])

    def mixer(g):
        for dx in range(1, XN):
            await_bytes(xbuf.at[dx, pl.ds(2 * g, 2)], xf_r.at[dx - 1, g])
        for i in range(2 * XN):
            dx, p = i // 2, 2 * g + i % 2
            block = xbuf[dx, p].astype(F32)
            for j in range(TN):
                xs[SUB * i : SUB * (i + 1), DB * j : DB * (j + 1)] = block[j]
        sec = xs[...]
        scale_two = lax.rsqrt(jnp.sum(sec * sec, axis=-1, keepdims=True) * (1.0 / D) + EPS)
        scaled = (sec * gains[...]).astype(BF16)
        preact = jnp.dot(scaled, upb[...], preferred_element_type=F32)
        hidden = jnp.square(jnp.maximum(preact * scale_two, 0.0)).astype(BF16)
        for j in range(TN):
            os[:, DB * j : DB * (j + 1)] = jnp.dot(hidden, dnb[j], preferred_element_type=F32)
        for i in range(2 * XN):
            dx, p = i // 2, 2 * g + i % 2
            for j in range(TN):
                block = os[SUB * i : SUB * (i + 1), DB * j : DB * (j + 1)]
                if dx == 0:
                    own[p, j] = block
                else:
                    rsx_s[dx - 1, p, j] = block.astype(BF16)
        pair = pl.ds(2 * g, 2)
        for dx in range(1, XN):
            send(
                rsx_s.at[dx - 1, pair], rsx_r.at[(-dx) % XN - 1, pair],
                rx_s.at[dx - 1, g], rx_r.at[(-dx) % XN - 1, g], zx(0, dx), t,
            )

    def sum_x(g):
        pair = pl.ds(2 * g, 2)
        for dx in range(1, XN):
            await_bytes(rsx_r.at[dx - 1, pair], rx_r.at[dx - 1, g])
        for p in (2 * g, 2 * g + 1):
            total = own[p]
            for dx in range(1, XN):
                total += rsx_r[dx - 1, p].astype(F32)
            zs[p] = total.astype(BF16)
            dz = ZORD[p]
            there = ZPOS[(-dz) % ZN]
            if dz == 0:
                pltpu.make_async_copy(zs.at[p, t], fin.at[0, t], fi_r.at[0]).start()
            for dy, dc in TPO if dz == 0 else TPO + ((0, 0),):
                s = tp_at(dy, dc)
                remote(
                    zs.at[p, s], fin.at[there, t], fi_s.at[p], fi_r.at[there], zx(dz, 0), s
                ).start()

    mixer(0)
    for g in range(1, GROUPS):
        mixer(g)
        sum_x(g - 1)
    sum_x(GROUPS - 1)

    total = jnp.zeros((TN, SUB, DB), F32)
    for p in range(ZN):
        await_bytes(fin.at[p], fi_r.at[p])
        total += fin[p].astype(F32)
    for s in range(TN):
        of[SUB * s : SUB * (s + 1), :] = total[s]
    out_ref[...] = (secf[...] + of[...]).astype(BF16)

    for src, sem in pending:
        await_bytes(src, sem)
    for p in range(ZN):
        count = TN - 1 if p == 0 else TN
        await_bytes(seg.at[pl.ds(0, count)], az_s.at[p])
        await_bytes(zs.at[p, pl.ds(0, count)], fi_s.at[p])
    store_mem.wait()


def write_out(*refs):
    ins, outs, sems = refs[:4], refs[4:8], refs[8]
    copies = [pltpu.make_async_copy(src, dst, sems.at[k]) for k, (src, dst) in enumerate(zip(ins, outs))]
    for copy in copies:
        copy.start()
    for copy in copies:
        copy.wait()


def per_device(
    tokens, memory, normalizer, stabilizer, norm_gain, query_weight, key_weight, value_weight, outgate_weight,
    input_gate_weight, forget_gate_weight, forget_bias, memory_gain, proj_weight, ffn_gain, up_weight, down_weight,
):
    hbm = pl.BlockSpec(memory_space=pltpu.HBM)
    anywhere = pl.BlockSpec(memory_space=pl.ANY)
    vmem = pl.BlockSpec(memory_space=pltpu.VMEM)
    dma = pltpu.SemaphoreType.DMA
    outs = (
        jax.ShapeDtypeStruct((ROWS, DB), BF16),
        jax.ShapeDtypeStruct((ROWS, DK, DK), F32),
        jax.ShapeDtypeStruct((ROWS, DK), F32),
        jax.ShapeDtypeStruct((1, ROWS), F32),
    )
    layer_out, memory_new, normalizer_new, stab_new = pl.pallas_call(
        kernel,
        out_shape=outs,
        in_specs=[hbm] * 17,
        out_specs=(vmem, anywhere, vmem, vmem),
        scratch_shapes=[
            pltpu.VMEM((ROWS, D), BF16),
            pltpu.VMEM((ROWS, DK, DK), F32),
            pltpu.VMEM((ROWS, DK), F32),
            pltpu.VMEM((1, ROWS), F32),
            pltpu.VMEM((1, D), F32),
            pltpu.VMEM((D, 4 * DK), BF16),
            pltpu.VMEM((TN, D), BF16),
            pltpu.VMEM((TN, D), BF16),
            pltpu.VMEM((1, TN), F32),
            pltpu.VMEM((1, DK), F32),
            pltpu.VMEM((TN * DK, DB), BF16),
            pltpu.VMEM((1, D), F32),
            pltpu.VMEM((D, FB), BF16),
            pltpu.VMEM((TN, FB, DB), BF16),
            pltpu.VMEM((ROWS, D), BF16),
            pltpu.VMEM((ROWS, DK), F32),
            pltpu.VMEM((2, ROWS, DK), F32),
            pltpu.VMEM((DK, DK), F32),
            pltpu.VMEM((ROWS, TN * DK), BF16),
            pltpu.VMEM((ROWS, DB), F32),
            pltpu.VMEM((TN, SUB, DB), BF16),
            pltpu.VMEM((XN, ZN, TN, SUB, DB), BF16),
            pltpu.VMEM((ROWS, D), F32),
            pltpu.VMEM((ROWS, D), F32),
            pltpu.VMEM((XN - 1, ZN, TN, SUB, DB), BF16),
            pltpu.VMEM((XN - 1, ZN, TN, SUB, DB), BF16),
            pltpu.VMEM((ZN, TN, SUB, DB), F32),
            pltpu.VMEM((ZN, TN, SUB, DB), BF16),
            pltpu.VMEM((ZN, TN, SUB, DB), BF16),
            pltpu.VMEM((ROWS, DB), F32),
            dma((18,)),
            dma((7,)), dma((7,)),
            dma((7,)), dma((7,)),
            dma((7,)), dma((7,)),
            dma((2, 7)), dma((2, 7)),
            dma((ZN,)), dma((ZN,)),
            dma((XN - 1, GROUPS)), dma((XN - 1, GROUPS)),
            dma((XN - 1, GROUPS)), dma((XN - 1, GROUPS)),
            dma((ZN,)), dma((ZN,)),
            pltpu.SemaphoreType.REGULAR,
        ],
        compiler_params=pltpu.CompilerParams(
            collective_id=0, has_side_effects=True, vmem_limit_bytes=40 * 1024 * 1024
        ),
        name="layer",
    )(
        *(
            pltpu.with_memory_space_constraint(a, pltpu.HBM)
            for a in (
                tokens,
                memory.reshape(ROWS, DK, DK),
                normalizer.reshape(ROWS, DK),
                stabilizer.T,
                norm_gain.reshape(1, D),
                query_weight, key_weight, value_weight, outgate_weight,
                input_gate_weight.T,
                forget_gate_weight.T,
                forget_bias.reshape(1, TN),
                memory_gain.reshape(1, DK),
                proj_weight,
                ffn_gain.reshape(1, DB),
                up_weight,
                down_weight,
            )
        )
    )
    layer_out, memory_new, normalizer_new, stab_new = pl.pallas_call(
        write_out,
        out_shape=outs,
        in_specs=[anywhere] * 4,
        out_specs=(hbm,) * 4,
        scratch_shapes=[dma((4,))],
        compiler_params=pltpu.CompilerParams(vmem_limit_bytes=4 * 1024 * 1024),
        name="write_out",
    )(layer_out, memory_new, normalizer_new, stab_new)
    return (
        layer_out,
        memory_new.reshape(ROWS, 1, DK, DK),
        normalizer_new.reshape(ROWS, 1, DK),
        stab_new.T,
    )


def solution(mesh):
    placed = (
        P("kv", "tp"),
        P("kv", "tp", None, None),
        P("kv", "tp", None),
        P("kv", "tp"),
        P(),
        P(None, "tp"),
        P(None, "tp"),
        P(None, "tp"),
        P(None, "tp"),
        P(),
        P(),
        P(),
        P("tp"),
        P(None, "tp"),
        P("tp"),
        P("tp", "kv"),
        P("kv", "tp"),
    )
    outs = (P("kv", "tp"), P("kv", "tp", None, None), P("kv", "tp", None), P("kv", "tp"))
    return jax.shard_map(per_device, mesh=mesh, in_specs=placed, out_specs=outs, check_vma=False)
```

```python
import jax
import jax.numpy as jnp
from jax import lax
from jax.experimental import pallas as pl
from jax.experimental.pallas import tpu as pltpu
from jax.sharding import PartitionSpec as P

D = 2048
DK = 128
EPS = 1e-06
XN = 4
ZN = 8
YN = 4
TN = 8
ROWS = 32
DB = D // TN
SUB = ROWS // TN
FB = 256
ZORD = (7, 2, 6, 3, 5, 4, 1, 0)
ZSEND = (0, 1, 7, 2, 6, 3, 5, 4)
ZPOS = tuple(ZORD.index(o) for o in range(ZN))
TPO = ((2, 0), (2, 1), (1, 0), (1, 1), (3, 0), (3, 1), (0, 1))
GROUPS = ZN // 2
F32 = jnp.float32
BF16 = jnp.bfloat16
MESH = pl.DeviceIdType.MESH


def remote(src, dst, send_sem, recv_sem, kv, tp):
    return pltpu.make_async_remote_copy(
        src_ref=src,
        dst_ref=dst,
        send_sem=send_sem,
        recv_sem=recv_sem,
        device_id={"kv": kv, "tp": tp},
        device_id_type=MESH,
    )


def await_bytes(ref, sem):
    pltpu.make_async_copy(ref, ref, sem).wait()


def kernel(
    tok_h, mem_h, nrm_h, stab_h, ng_h, qw_h, kw_h, vw_h, ow_h, ig_h, fg_h, fb_h, mg_h, pw_h, gain_h, up_h, dn_h,
    out_ref, memn_h, nrmn_ref, stabn_ref,
    tk, mem, nrm, stab, ng, qkvo, ig, fg, fb, mg, pw, gains, upb, dnb,
    nb, qf, colrow, colmat, mx, secf, seg, xbuf, xs, os, rsx_s, rsx_r, own, zs, fin, of,
    lsem, tok_s, tok_r, gain_s, gain_r, mix_s, mix_r, w_s, w_r, az_s, az_r, xf_s, xf_r, rx_s, rx_r, fi_s, fi_r,
    zready,
):
    kv = lax.axis_index("kv")
    t = lax.axis_index("tp")
    z, x = kv // XN, kv % XN
    y, c = t // 2, t % 2

    def zx(dz, dx):
        return ((z + dz) % ZN) * XN + (x + dx) % XN

    def tp_at(dy, dc):
        return ((y + dy) % YN) * 2 + (c + dc) % 2

    pending = []

    def send(src, dst, ssem, rsem, kv_to, tp_to):
        remote(src, dst, ssem, rsem, kv_to, tp_to).start()
        pending.append((src, ssem))

    lane_t = pl.ds(pl.multiple_of(t * DB, DB), DB)
    lane_h = pl.ds(pl.multiple_of(t * DK, DK), DK)
    row_t = lane_t

    loads = {}

    def load(name, src, dst):
        k = len(loads)
        loads[name] = pltpu.make_async_copy(src, dst, lsem.at[k])
        loads[name].start()

    load("tok", tok_h, tk.at[:, lane_t])
    load("gain", gain_h, gains.at[:, lane_t])
    load("up", up_h, upb.at[row_t])
    load("dn", dn_h, dnb.at[t])
    load("ng", ng_h, ng)
    for k, (name, w) in enumerate((("q", qw_h), ("k", kw_h), ("v", vw_h), ("o", ow_h))):
        load(name, w, qkvo.at[:, DK * k : DK * (k + 1)])
    load("ig", ig_h, ig)
    load("fg", fg_h, fg)
    load("fb", fb_h, fb)
    load("stab", stab_h, stab)
    load("nrm", nrm_h, nrm)
    load("mem", mem_h, mem)
    load("mg", mg_h, mg)
    load("pw", pw_h, pw)

    barrier = pltpu.get_barrier_semaphore()
    for dy, dc in TPO:
        pl.semaphore_signal(barrier, inc=1, device_id={"kv": kv, "tp": tp_at(dy, dc)}, device_id_type=MESH)
    for dx in range(1, XN):
        pl.semaphore_signal(barrier, inc=1, device_id={"kv": zx(0, dx), "tp": t}, device_id_type=MESH)
    for dz in range(1, ZN):
        pl.semaphore_signal(barrier, inc=1, device_id={"kv": zx(dz, 0), "tp": t}, device_id_type=MESH)
    pl.semaphore_wait(barrier, 7 + (XN - 1) + (ZN - 1))
    for dz in range(1, ZN):
        pl.semaphore_signal(zready, inc=1, device_id={"kv": zx(dz, 0), "tp": t}, device_id_type=MESH)

    loads["tok"].wait()
    for k, (dy, dc) in enumerate(TPO):
        send(tk.at[:, lane_t], tk.at[:, lane_t], tok_s.at[k], tok_r.at[k], kv, tp_at(dy, dc))
    loads["gain"].wait()
    for k, (dy, dc) in enumerate(TPO):
        send(gains.at[:, lane_t], gains.at[:, lane_t], gain_s.at[k], gain_r.at[k], kv, tp_at(dy, dc))

    def w_slot(m, dy, dc):
        s = tp_at(dy, dc)
        return upb.at[pl.ds(pl.multiple_of(s * DB, DB), DB)] if m == 0 else dnb.at[s]

    loads["up"].wait()
    send(w_slot(0, 0, 0), w_slot(0, 0, 0), w_s.at[0, 0], w_r.at[0, 0], kv, tp_at(1, 0))
    send(w_slot(0, 0, 0), w_slot(0, 0, 0), w_s.at[0, 1], w_r.at[0, 1], kv, tp_at(3, 0))
    send(w_slot(0, 0, 0), w_slot(0, 0, 0), w_s.at[0, 3], w_r.at[0, 3], kv, tp_at(0, 1))

    for name in ("ng", "q", "k", "v", "o", "ig", "fg", "fb", "stab", "nrm"):
        loads[name].wait()
    for k, (dy, dc) in enumerate(TPO):
        s = tp_at(-dy, -dc)
        await_bytes(tk.at[:, pl.ds(pl.multiple_of(s * DB, DB), DB)], tok_r.at[k])
    rows = tk[...].astype(F32)
    scale_one = lax.rsqrt(jnp.sum(rows * rows, axis=-1, keepdims=True) * (1.0 / D) + EPS)
    nb[...] = (rows * scale_one * ng[...]).astype(BF16)
    proj4 = jnp.dot(nb[...], qkvo[...], preferred_element_type=F32).astype(BF16).astype(F32)
    query = proj4[:, :DK]
    keys = proj4[:, DK : 2 * DK] * DK ** (-0.5)
    values = proj4[:, 2 * DK : 3 * DK]
    gate_out = proj4[:, 3 * DK :]
    qf[...] = query

    contract = (((1,), (1,)), ((), ()))
    all_in = lax.dot_general(nb[...], ig[...], contract, preferred_element_type=F32)
    all_forget = lax.dot_general(nb[...], fg[...], contract, preferred_element_type=F32) + fb[...]
    head = lax.broadcasted_iota(jnp.int32, (ROWS, TN), 1) == t
    input_log = jnp.sum(jnp.where(head, all_in, 0.0), axis=1, keepdims=True)
    raw = jnp.sum(jnp.where(head, all_forget, 0.0), axis=1, keepdims=True)
    forget_log = jnp.minimum(raw, 0.0) - jnp.log1p(jnp.exp(-jnp.abs(raw)))
    diag = lax.broadcasted_iota(jnp.int32, (ROWS, ROWS), 0) == lax.broadcasted_iota(jnp.int32, (ROWS, ROWS), 1)
    stab_col = jnp.sum(jnp.where(diag, jnp.broadcast_to(stab[...], (ROWS, ROWS)), 0.0), axis=1, keepdims=True)
    stab_new = jnp.maximum(forget_log + stab_col, input_log)
    keep = jnp.exp(forget_log + stab_col - stab_new)
    admit = jnp.exp(input_log - stab_new)
    normalizer_new = keep * nrm[...] + admit * keys
    denom = jnp.sum(normalizer_new * query, axis=1, keepdims=True)
    key_query = jnp.sum(keys * query, axis=1, keepdims=True)

    loads["mem"].wait()
    lane = lax.broadcasted_iota(jnp.int32, (DK, DK), 1)

    def read_memory(b, acc):
        part = jnp.sum(mem[b] * qf[pl.ds(b, 1), :], axis=1, keepdims=True)
        return jnp.where(lane == b, part, acc)

    read = lax.fori_loop(0, ROWS, read_memory, jnp.zeros((DK, DK), F32), unroll=ROWS)
    memory_query = read.T[:ROWS, :]
    numer = keep * memory_query + (admit * key_query) * values
    cell = numer / jnp.maximum(jnp.abs(denom), 1.0)
    loads["mg"].wait()
    mx[:, lane_h] = (cell * mg[...] * jax.nn.sigmoid(gate_out)).astype(BF16)
    for k, (dy, dc) in enumerate(TPO):
        send(mx.at[:, lane_h], mx.at[:, lane_h], mix_s.at[k], mix_r.at[k], kv, tp_at(dy, dc))

    loads["dn"].wait()
    send(w_slot(1, 0, 0), w_slot(1, 0, 0), w_s.at[1, 0], w_r.at[1, 0], kv, tp_at(1, 0))
    send(w_slot(1, 0, 0), w_slot(1, 0, 0), w_s.at[1, 1], w_r.at[1, 1], kv, tp_at(3, 0))
    send(w_slot(1, 0, 0), w_slot(1, 0, 0), w_s.at[1, 3], w_r.at[1, 3], kv, tp_at(0, 1))

    nrmn_ref[...] = normalizer_new
    stabn_ref[...] = jnp.sum(
        jnp.where(diag, jnp.broadcast_to(stab_new, (ROWS, ROWS)), 0.0), axis=0, keepdims=True
    )
    colrow[0] = jnp.broadcast_to(keep, (ROWS, DK))
    colrow[1] = keys
    colmat[:ROWS, :] = admit * values
    colmat[ROWS:, :] = jnp.zeros((DK - ROWS, DK), F32)
    admitted = colmat[...].T

    def write_memory(b, carry):
        column = jnp.sum(jnp.where(lane == b, admitted, 0.0), axis=1, keepdims=True)
        mem[b] = colrow[0, pl.ds(b, 1), :] * mem[b] + column * colrow[1, pl.ds(b, 1), :]
        return carry

    lax.fori_loop(0, ROWS, write_memory, 0, unroll=ROWS)
    store_mem = pltpu.make_async_copy(mem, memn_h, lsem.at[len(loads)])
    store_mem.start()

    loads["pw"].wait()
    for k, (dy, dc) in enumerate(TPO):
        s = tp_at(-dy, -dc)
        await_bytes(mx.at[:, pl.ds(pl.multiple_of(s * DK, DK), DK)], mix_r.at[k])
    projected = jnp.dot(mx[...], pw[...], preferred_element_type=F32)
    second = (tk[:, lane_t].astype(F32) + projected).astype(BF16).astype(F32)
    secf[...] = second
    for s in range(TN):
        seg[s] = secf[SUB * s : SUB * (s + 1), :].astype(BF16)

    pl.semaphore_wait(zready, ZN - 1)
    home = ZPOS[0]
    pltpu.make_async_copy(seg.at[t], xbuf.at[0, home, t], az_r.at[home]).start()
    for dz in ZSEND:
        there = ZPOS[(-dz) % ZN]
        for dy, dc in TPO if dz == 0 else TPO + ((0, 0),):
            s = tp_at(dy, dc)
            remote(
                seg.at[s], xbuf.at[0, there, t], az_s.at[ZPOS[dz]], az_r.at[there], zx(dz, 0), s
            ).start()

    def relay(m, k, dy, forward):
        slot = w_slot(m, dy, 0)
        await_bytes(slot, w_r.at[m, k])
        if forward is not None:
            send(slot, slot, w_s.at[m, 2], w_r.at[m, 2], kv, tp_at(forward, 0))
        send(slot, slot, w_s.at[m, 4 + k], w_r.at[m, 4 + k], kv, tp_at(0, 1))

    relay(0, 0, 3, 1)
    relay(1, 1, 1, 3)
    relay(0, 1, 1, None)
    relay(1, 0, 3, None)

    for dz in ZSEND:
        p = ZPOS[dz]
        await_bytes(xbuf.at[0, p], az_r.at[p])
        for dx in range(1, XN):
            send(
                xbuf.at[0, p], xbuf.at[(-dx) % XN, p],
                xf_s.at[dx - 1, p], xf_r.at[(-dx) % XN - 1, p], zx(0, dx), t,
            )

    relay(0, 2, 2, None)
    relay(1, 2, 2, None)
    for k, (dy, dc) in enumerate(TPO):
        s = tp_at(-dy, -dc)
        await_bytes(gains.at[:, pl.ds(pl.multiple_of(s * DB, DB), DB)], gain_r.at[k])
    for m in range(2):
        for k, dy in ((3, 0), (4, 3), (5, 1), (6, 2)):
            await_bytes(w_slot(m, dy, 1), w_r.at[m, k])

    def mixer(g):
        for dx in range(1, XN):
            for p in (2 * g, 2 * g + 1):
                await_bytes(xbuf.at[dx, p], xf_r.at[dx - 1, p])
        for i in range(2 * XN):
            dx, p = i // 2, 2 * g + i % 2
            block = xbuf[dx, p].astype(F32)
            for j in range(TN):
                xs[SUB * i : SUB * (i + 1), DB * j : DB * (j + 1)] = block[j]
        sec = xs[...]
        scale_two = lax.rsqrt(jnp.sum(sec * sec, axis=-1, keepdims=True) * (1.0 / D) + EPS)
        scaled = (sec * gains[...]).astype(BF16)
        preact = jnp.dot(scaled, upb[...], preferred_element_type=F32)
        hidden = jnp.square(jnp.maximum(preact * scale_two, 0.0)).astype(BF16)
        for j in range(TN):
            os[:, DB * j : DB * (j + 1)] = jnp.dot(hidden, dnb[j], preferred_element_type=F32)
        for i in range(2 * XN):
            dx, p = i // 2, 2 * g + i % 2
            for j in range(TN):
                block = os[SUB * i : SUB * (i + 1), DB * j : DB * (j + 1)]
                if dx == 0:
                    own[p, j] = block
                else:
                    rsx_s[dx - 1, p, j] = block.astype(BF16)
        pair = pl.ds(2 * g, 2)
        for dx in range(1, XN):
            send(
                rsx_s.at[dx - 1, pair], rsx_r.at[(-dx) % XN - 1, pair],
                rx_s.at[dx - 1, g], rx_r.at[(-dx) % XN - 1, g], zx(0, dx), t,
            )

    def sum_x(g):
        pair = pl.ds(2 * g, 2)
        for dx in range(1, XN):
            await_bytes(rsx_r.at[dx - 1, pair], rx_r.at[dx - 1, g])
        for p in (2 * g, 2 * g + 1):
            total = own[p]
            for dx in range(1, XN):
                total += rsx_r[dx - 1, p].astype(F32)
            zs[p] = total.astype(BF16)
            dz = ZORD[p]
            there = ZPOS[(-dz) % ZN]
            if dz == 0:
                pltpu.make_async_copy(zs.at[p, t], fin.at[home, t], fi_r.at[home]).start()
            for dy, dc in TPO if dz == 0 else TPO + ((0, 0),):
                s = tp_at(dy, dc)
                remote(
                    zs.at[p, s], fin.at[there, t], fi_s.at[p], fi_r.at[there], zx(dz, 0), s
                ).start()

    for g in range(GROUPS):
        mixer(g)
    for g in range(GROUPS):
        sum_x(g)

    total = jnp.zeros((TN, SUB, DB), F32)
    for p in range(ZN):
        await_bytes(fin.at[p], fi_r.at[p])
        total += fin[p].astype(F32)
    for s in range(TN):
        of[SUB * s : SUB * (s + 1), :] = total[s]
    out_ref[...] = (secf[...] + of[...]).astype(BF16)

    for src, sem in pending:
        await_bytes(src, sem)
    for p in range(ZN):
        count = TN - 1 if p == home else TN
        await_bytes(seg.at[pl.ds(0, count)], az_s.at[p])
        await_bytes(zs.at[p, pl.ds(0, count)], fi_s.at[p])
    store_mem.wait()


def write_out(*refs):
    ins, outs, sems = refs[:4], refs[4:8], refs[8]
    copies = [pltpu.make_async_copy(src, dst, sems.at[k]) for k, (src, dst) in enumerate(zip(ins, outs))]
    for copy in copies:
        copy.start()
    for copy in copies:
        copy.wait()


def per_device(
    tokens, memory, normalizer, stabilizer, norm_gain, query_weight, key_weight, value_weight, outgate_weight,
    input_gate_weight, forget_gate_weight, forget_bias, memory_gain, proj_weight, ffn_gain, up_weight, down_weight,
):
    hbm = pl.BlockSpec(memory_space=pltpu.HBM)
    anywhere = pl.BlockSpec(memory_space=pl.ANY)
    vmem = pl.BlockSpec(memory_space=pltpu.VMEM)
    dma = pltpu.SemaphoreType.DMA
    outs = (
        jax.ShapeDtypeStruct((ROWS, DB), BF16),
        jax.ShapeDtypeStruct((ROWS, DK, DK), F32),
        jax.ShapeDtypeStruct((ROWS, DK), F32),
        jax.ShapeDtypeStruct((1, ROWS), F32),
    )
    layer_out, memory_new, normalizer_new, stab_new = pl.pallas_call(
        kernel,
        out_shape=outs,
        in_specs=[hbm] * 17,
        out_specs=(vmem, anywhere, vmem, vmem),
        scratch_shapes=[
            pltpu.VMEM((ROWS, D), BF16),
            pltpu.VMEM((ROWS, DK, DK), F32),
            pltpu.VMEM((ROWS, DK), F32),
            pltpu.VMEM((1, ROWS), F32),
            pltpu.VMEM((1, D), F32),
            pltpu.VMEM((D, 4 * DK), BF16),
            pltpu.VMEM((TN, D), BF16),
            pltpu.VMEM((TN, D), BF16),
            pltpu.VMEM((1, TN), F32),
            pltpu.VMEM((1, DK), F32),
            pltpu.VMEM((TN * DK, DB), BF16),
            pltpu.VMEM((1, D), F32),
            pltpu.VMEM((D, FB), BF16),
            pltpu.VMEM((TN, FB, DB), BF16),
            pltpu.VMEM((ROWS, D), BF16),
            pltpu.VMEM((ROWS, DK), F32),
            pltpu.VMEM((2, ROWS, DK), F32),
            pltpu.VMEM((DK, DK), F32),
            pltpu.VMEM((ROWS, TN * DK), BF16),
            pltpu.VMEM((ROWS, DB), F32),
            pltpu.VMEM((TN, SUB, DB), BF16),
            pltpu.VMEM((XN, ZN, TN, SUB, DB), BF16),
            pltpu.VMEM((ROWS, D), F32),
            pltpu.VMEM((ROWS, D), F32),
            pltpu.VMEM((XN - 1, ZN, TN, SUB, DB), BF16),
            pltpu.VMEM((XN - 1, ZN, TN, SUB, DB), BF16),
            pltpu.VMEM((ZN, TN, SUB, DB), F32),
            pltpu.VMEM((ZN, TN, SUB, DB), BF16),
            pltpu.VMEM((ZN, TN, SUB, DB), BF16),
            pltpu.VMEM((ROWS, DB), F32),
            dma((18,)),
            dma((7,)), dma((7,)),
            dma((7,)), dma((7,)),
            dma((7,)), dma((7,)),
            dma((2, 7)), dma((2, 7)),
            dma((ZN,)), dma((ZN,)),
            dma((XN - 1, ZN)), dma((XN - 1, ZN)),
            dma((XN - 1, GROUPS)), dma((XN - 1, GROUPS)),
            dma((ZN,)), dma((ZN,)),
            pltpu.SemaphoreType.REGULAR,
        ],
        compiler_params=pltpu.CompilerParams(
            collective_id=0, has_side_effects=True, vmem_limit_bytes=40 * 1024 * 1024
        ),
        name="layer",
    )(
        *(
            pltpu.with_memory_space_constraint(a, pltpu.HBM)
            for a in (
                tokens,
                memory.reshape(ROWS, DK, DK),
                normalizer.reshape(ROWS, DK),
                stabilizer.T,
                norm_gain.reshape(1, D),
                query_weight, key_weight, value_weight, outgate_weight,
                input_gate_weight.T,
                forget_gate_weight.T,
                forget_bias.reshape(1, TN),
                memory_gain.reshape(1, DK),
                proj_weight,
                ffn_gain.reshape(1, DB),
                up_weight,
                down_weight,
            )
        )
    )
    layer_out, memory_new, normalizer_new, stab_new = pl.pallas_call(
        write_out,
        out_shape=outs,
        in_specs=[anywhere] * 4,
        out_specs=(hbm,) * 4,
        scratch_shapes=[dma((4,))],
        compiler_params=pltpu.CompilerParams(vmem_limit_bytes=4 * 1024 * 1024),
        name="write_out",
    )(layer_out, memory_new, normalizer_new, stab_new)
    return (
        layer_out,
        memory_new.reshape(ROWS, 1, DK, DK),
        normalizer_new.reshape(ROWS, 1, DK),
        stab_new.T,
    )


def solution(mesh):
    placed = (
        P("kv", "tp"),
        P("kv", "tp", None, None),
        P("kv", "tp", None),
        P("kv", "tp"),
        P(),
        P(None, "tp"),
        P(None, "tp"),
        P(None, "tp"),
        P(None, "tp"),
        P(),
        P(),
        P(),
        P("tp"),
        P(None, "tp"),
        P("tp"),
        P("tp", "kv"),
        P("kv", "tp"),
    )
    outs = (P("kv", "tp"), P("kv", "tp", None, None), P("kv", "tp", None), P("kv", "tp"))
    return jax.shard_map(per_device, mesh=mesh, in_specs=placed, out_specs=outs, check_vma=False)
```

```python
import jax
import jax.numpy as jnp
from jax import lax
from jax.experimental import pallas as pl
from jax.experimental.pallas import tpu as pltpu
from jax.sharding import PartitionSpec as P

D = 2048
DK = 128
EPS = 1e-06
XN = 4
ZN = 8
YN = 4
TN = 8
ROWS = 32
DB = D // TN
SUB = ROWS // TN
FB = 256
ZORD = (0, 1, 7, 2, 6, 3, 5, 4)
ZSEND = (0, 1, 7, 2, 6, 3, 5, 4)
DIRECT_IN = ()
DIRECT_OUT = (4,)
ORDER = (
    "f0", "f1", "f7", "f2", "f6", "r0", "r1", "f3", "f5", "f4", "r2", "r3", "w",
    "m0", "m72", "m63", "m54", "m1", "s0", "s7", "s2", "s6", "s3", "s5", "s1",
)
ZPOS = tuple(ZORD.index(o) for o in range(ZN))
TPO = ((2, 0), (2, 1), (1, 0), (1, 1), (3, 0), (3, 1), (0, 1))
F32 = jnp.float32
BF16 = jnp.bfloat16
MESH = pl.DeviceIdType.MESH


def remote(src, dst, send_sem, recv_sem, kv, tp):
    return pltpu.make_async_remote_copy(
        src_ref=src,
        dst_ref=dst,
        send_sem=send_sem,
        recv_sem=recv_sem,
        device_id={"kv": kv, "tp": tp},
        device_id_type=MESH,
    )


def await_bytes(ref, sem):
    pltpu.make_async_copy(ref, ref, sem).wait()


def kernel(
    tok_h, mem_h, nrm_h, stab_h, ng_h, qw_h, kw_h, vw_h, ow_h, ig_h, fg_h, fb_h, mg_h, pw_h, gain_h, up_h, dn_h,
    out_ref, memn_h, nrmn_ref, stabn_ref,
    tk, mem, nrm, stab, ng, qkvo, ig, fg, fb, mg, pw, gains, upb, dnb,
    nb, qf, colrow, colmat, mx, secf, seg, xbuf, xs, os, rsx_s, rsx_r, own, zs, fin, of,
    lsem, tok_s, tok_r, gain_s, gain_r, mix_s, mix_r, w_s, w_r, az_s, az_r, xf_s, xf_r, rx_s, rx_r, fi_s, fi_r,
    zready, xready,
):
    kv = lax.axis_index("kv")
    t = lax.axis_index("tp")
    z, x = kv // XN, kv % XN
    y, c = t // 2, t % 2

    def zx(dz, dx):
        return ((z + dz) % ZN) * XN + (x + dx) % XN

    def tp_at(dy, dc):
        return ((y + dy) % YN) * 2 + (c + dc) % 2

    pending = []

    def send(src, dst, ssem, rsem, kv_to, tp_to):
        remote(src, dst, ssem, rsem, kv_to, tp_to).start()
        pending.append((src, ssem))

    lane_t = pl.ds(pl.multiple_of(t * DB, DB), DB)
    lane_h = pl.ds(pl.multiple_of(t * DK, DK), DK)
    row_t = lane_t

    loads = {}

    def load(name, src, dst):
        k = len(loads)
        loads[name] = pltpu.make_async_copy(src, dst, lsem.at[k])
        loads[name].start()

    load("tok", tok_h, tk.at[:, lane_t])
    load("gain", gain_h, gains.at[:, lane_t])
    load("up", up_h, upb.at[row_t])
    load("dn", dn_h, dnb.at[t])
    load("ng", ng_h, ng)
    for k, (name, w) in enumerate((("q", qw_h), ("k", kw_h), ("v", vw_h), ("o", ow_h))):
        load(name, w, qkvo.at[:, DK * k : DK * (k + 1)])
    load("ig", ig_h, ig)
    load("fg", fg_h, fg)
    load("fb", fb_h, fb)
    load("stab", stab_h, stab)
    load("nrm", nrm_h, nrm)
    load("mem", mem_h, mem)
    load("mg", mg_h, mg)
    load("pw", pw_h, pw)

    def tell(sem, kv_to, tp_to):
        pl.semaphore_signal(sem, inc=1, device_id={"kv": kv_to, "tp": tp_to}, device_id_type=MESH)

    barrier = pltpu.get_barrier_semaphore()
    for dy, dc in TPO:
        tell(barrier, kv, tp_at(dy, dc))
    for step in (1, -1):
        tell(barrier, zx(0, step), t)
        tell(barrier, zx(step, 0), t)
    pl.semaphore_wait(barrier, 7 + 4)
    for step in (1, -1):
        tell(xready.at[0], zx(0, step), t)
        tell(zready.at[0], zx(step, 0), t)

    loads["tok"].wait()
    for k, (dy, dc) in enumerate(TPO):
        send(tk.at[:, lane_t], tk.at[:, lane_t], tok_s.at[k], tok_r.at[k], kv, tp_at(dy, dc))
    loads["gain"].wait()
    for k, (dy, dc) in enumerate(TPO):
        send(gains.at[:, lane_t], gains.at[:, lane_t], gain_s.at[k], gain_r.at[k], kv, tp_at(dy, dc))

    def w_slot(m, dy, dc):
        s = tp_at(dy, dc)
        if m < 2:
            return upb.at[pl.ds(pl.multiple_of(s * DB + DB // 2 * m, DB // 2), DB // 2)]
        return dnb.at[s, pl.ds(FB // 2 * (m - 2), FB // 2)]

    def send_weights(m):
        slot = w_slot(m, 0, 0)
        for k, (dy, dc) in ((0, (1, 0)), (1, (3, 0)), (3, (0, 1))):
            send(slot, slot, w_s.at[m, k], w_r.at[m, k], kv, tp_at(dy, dc))

    loads["up"].wait()
    send_weights(0)
    send_weights(1)

    pl.semaphore_wait(xready.at[0], 2)
    pl.semaphore_wait(zready.at[0], 2)
    for step in (2, -2):
        tell(zready.at[1], zx(step, 0), t)

    for name in ("ng", "q", "k", "v", "o", "ig", "fg", "fb", "stab", "nrm"):
        loads[name].wait()
    for k, (dy, dc) in enumerate(TPO):
        s = tp_at(-dy, -dc)
        await_bytes(tk.at[:, pl.ds(pl.multiple_of(s * DB, DB), DB)], tok_r.at[k])
    pl.semaphore_wait(zready.at[1], 2)
    for step in (3, -3, 4):
        tell(zready.at[2], zx(step, 0), t)
    rows = tk[...].astype(F32)
    scale_one = lax.rsqrt(jnp.sum(rows * rows, axis=-1, keepdims=True) * (1.0 / D) + EPS)
    nb[...] = (rows * scale_one * ng[...]).astype(BF16)
    proj4 = jnp.dot(nb[...], qkvo[...], preferred_element_type=F32).astype(BF16).astype(F32)
    query = proj4[:, :DK]
    keys = proj4[:, DK : 2 * DK] * DK ** (-0.5)
    values = proj4[:, 2 * DK : 3 * DK]
    gate_out = proj4[:, 3 * DK :]
    qf[...] = query

    contract = (((1,), (1,)), ((), ()))
    all_in = lax.dot_general(nb[...], ig[...], contract, preferred_element_type=F32)
    all_forget = lax.dot_general(nb[...], fg[...], contract, preferred_element_type=F32) + fb[...]
    head = lax.broadcasted_iota(jnp.int32, (ROWS, TN), 1) == t
    input_log = jnp.sum(jnp.where(head, all_in, 0.0), axis=1, keepdims=True)
    raw = jnp.sum(jnp.where(head, all_forget, 0.0), axis=1, keepdims=True)
    forget_log = jnp.minimum(raw, 0.0) - jnp.log1p(jnp.exp(-jnp.abs(raw)))
    diag = lax.broadcasted_iota(jnp.int32, (ROWS, ROWS), 0) == lax.broadcasted_iota(jnp.int32, (ROWS, ROWS), 1)
    stab_col = jnp.sum(jnp.where(diag, jnp.broadcast_to(stab[...], (ROWS, ROWS)), 0.0), axis=1, keepdims=True)
    stab_new = jnp.maximum(forget_log + stab_col, input_log)
    keep = jnp.exp(forget_log + stab_col - stab_new)
    admit = jnp.exp(input_log - stab_new)
    normalizer_new = keep * nrm[...] + admit * keys
    denom = jnp.sum(normalizer_new * query, axis=1, keepdims=True)
    key_query = jnp.sum(keys * query, axis=1, keepdims=True)

    loads["mem"].wait()
    lane = lax.broadcasted_iota(jnp.int32, (DK, DK), 1)

    def read_memory(b, acc):
        part = jnp.sum(mem[b] * qf[pl.ds(b, 1), :], axis=1, keepdims=True)
        return jnp.where(lane == b, part, acc)

    read = lax.fori_loop(0, ROWS, read_memory, jnp.zeros((DK, DK), F32), unroll=ROWS)
    memory_query = read.T[:ROWS, :]
    numer = keep * memory_query + (admit * key_query) * values
    cell = numer / jnp.maximum(jnp.abs(denom), 1.0)
    loads["mg"].wait()
    mx[:, lane_h] = (cell * mg[...] * jax.nn.sigmoid(gate_out)).astype(BF16)
    for k, (dy, dc) in enumerate(TPO):
        send(mx.at[:, lane_h], mx.at[:, lane_h], mix_s.at[k], mix_r.at[k], kv, tp_at(dy, dc))

    loads["dn"].wait()
    send_weights(2)
    send_weights(3)
    pl.semaphore_wait(zready.at[2], 3)
    for dx in range(1, XN):
        tell(xready.at[1], zx(0, dx), t)

    nrmn_ref[...] = normalizer_new
    stabn_ref[...] = jnp.sum(
        jnp.where(diag, jnp.broadcast_to(stab_new, (ROWS, ROWS)), 0.0), axis=0, keepdims=True
    )
    colrow[0] = jnp.broadcast_to(keep, (ROWS, DK))
    colrow[1] = keys
    colmat[:ROWS, :] = admit * values
    colmat[ROWS:, :] = jnp.zeros((DK - ROWS, DK), F32)
    admitted = colmat[...].T

    def write_memory(b, carry):
        column = jnp.sum(jnp.where(lane == b, admitted, 0.0), axis=1, keepdims=True)
        mem[b] = colrow[0, pl.ds(b, 1), :] * mem[b] + column * colrow[1, pl.ds(b, 1), :]
        return carry

    lax.fori_loop(0, ROWS, write_memory, 0, unroll=ROWS)
    store_mem = pltpu.make_async_copy(mem, memn_h, lsem.at[len(loads)])
    store_mem.start()

    def relay(m, k, dy, forward):
        slot = w_slot(m, dy, 0)
        await_bytes(slot, w_r.at[m, k])
        if forward is not None:
            send(slot, slot, w_s.at[m, 2], w_r.at[m, 2], kv, tp_at(forward, 0))
        send(slot, slot, w_s.at[m, 4 + k], w_r.at[m, 4 + k], kv, tp_at(0, 1))

    loads["pw"].wait()
    for k, (dy, dc) in enumerate(TPO):
        s = tp_at(-dy, -dc)
        await_bytes(mx.at[:, pl.ds(pl.multiple_of(s * DK, DK), DK)], mix_r.at[k])
    projected = jnp.dot(mx[...], pw[...], preferred_element_type=F32)
    second = (tk[:, lane_t].astype(F32) + projected).astype(BF16).astype(F32)
    secf[...] = second
    for s in range(TN):
        seg[s] = secf[SUB * s : SUB * (s + 1), :].astype(BF16)

    def scatter(dz, dx, src, dst, ssem, rsem):
        there = ZPOS[(-dz) % ZN]
        slot = (-dx) % XN
        for dy, dc in TPO + ((0, 0),):
            s = tp_at(dy, dc)
            if dz == 0 and dx == 0 and (dy, dc) == (0, 0):
                pltpu.make_async_copy(src.at[s], dst.at[slot, there, t], rsem.at[slot, there]).start()
            else:
                remote(
                    src.at[s], dst.at[slot, there, t], ssem.at[dx, ZPOS[dz]], rsem.at[slot, there], zx(dz, dx), s
                ).start()

    def targets(dz, direct):
        return range(XN) if dz in direct else (0,)

    pl.semaphore_wait(xready.at[1], XN - 1)
    for dz in ZSEND:
        for dx in targets(dz, DIRECT_IN):
            scatter(dz, dx, seg, xbuf, az_s, az_r)

    relay(0, 0, 3, 1)
    relay(1, 1, 1, 3)
    relay(0, 1, 1, None)
    relay(1, 0, 3, None)
    relay(2, 1, 1, 3)
    relay(3, 0, 3, 1)
    relay(2, 0, 3, None)
    relay(3, 1, 1, None)

    def forward(dz):
        p = ZPOS[dz]
        await_bytes(xbuf.at[0, p], az_r.at[0, p])
        for dx in range(1, XN):
            send(
                xbuf.at[0, p], xbuf.at[(-dx) % XN, p],
                xf_s.at[dx - 1, p], xf_r.at[(-dx) % XN - 1, p], zx(0, dx), t,
            )

    def rest_of_weights():
        for k, (dy, dc) in enumerate(TPO):
            s = tp_at(-dy, -dc)
            await_bytes(gains.at[:, pl.ds(pl.multiple_of(s * DB, DB), DB)], gain_r.at[k])
        for m in range(4):
            for k, dy in ((3, 0), (4, 3), (5, 1), (6, 2)):
                await_bytes(w_slot(m, dy, 1), w_r.at[m, k])

    def mixer(group):
        blocks = [(dx, ZPOS[dz]) for dx in range(XN) for dz in group]
        count = SUB * len(blocks)
        for dx, p in blocks:
            if ZORD[p] in DIRECT_IN:
                await_bytes(xbuf.at[dx, p], az_r.at[dx, p])
            elif dx > 0:
                await_bytes(xbuf.at[dx, p], xf_r.at[dx - 1, p])
        for i, (dx, p) in enumerate(blocks):
            block = xbuf[dx, p].astype(F32)
            for j in range(TN):
                xs[SUB * i : SUB * (i + 1), DB * j : DB * (j + 1)] = block[j]
        sec = xs[:count, :]
        scale_two = lax.rsqrt(jnp.sum(sec * sec, axis=-1, keepdims=True) * (1.0 / D) + EPS)
        scaled = (sec * gains[...]).astype(BF16)
        preact = jnp.dot(scaled, upb[...], preferred_element_type=F32)
        hidden = jnp.square(jnp.maximum(preact * scale_two, 0.0)).astype(BF16)
        for j in range(TN):
            os[:count, DB * j : DB * (j + 1)] = jnp.dot(hidden, dnb[j], preferred_element_type=F32)
        for i, (dx, p) in enumerate(blocks):
            for j in range(TN):
                block = os[SUB * i : SUB * (i + 1), DB * j : DB * (j + 1)]
                if dx == 0 and ZORD[p] not in DIRECT_OUT:
                    own[p, j] = block
                else:
                    rsx_s[dx, p, j] = block.astype(BF16)
        for dz in group:
            p = ZPOS[dz]
            if dz in DIRECT_OUT:
                for dx in range(XN):
                    scatter(dz, dx, rsx_s.at[dx, p], fin, fi_s, fi_r)
            else:
                for dx in range(1, XN):
                    send(
                        rsx_s.at[dx, p], rsx_r.at[(-dx) % XN - 1, p],
                        rx_s.at[dx - 1, p], rx_r.at[(-dx) % XN - 1, p], zx(0, dx), t,
                    )

    def sum_x(p):
        for dx in range(1, XN):
            await_bytes(rsx_r.at[dx - 1, p], rx_r.at[dx - 1, p])
        total = own[p]
        for dx in range(1, XN):
            total += rsx_r[dx - 1, p].astype(F32)
        zs[p] = total.astype(BF16)
        scatter(ZORD[p], 0, zs.at[p], fin, fi_s, fi_r)

    for step in ORDER:
        group = [int(digit) for digit in step[1:]]
        if step == "w":
            rest_of_weights()
        elif step[0] == "r":
            relay(group[0], 2, 2, None)
        elif step[0] == "f":
            forward(group[0])
        elif step[0] == "m":
            mixer(group)
        else:
            sum_x(ZPOS[group[0]])

    total = jnp.zeros((TN, SUB, DB), F32)
    for p in range(ZN):
        for dx in targets(ZORD[p], DIRECT_OUT):
            await_bytes(fin.at[dx, p], fi_r.at[dx, p])
            total += fin[dx, p].astype(F32)
    for s in range(TN):
        of[SUB * s : SUB * (s + 1), :] = total[s]
    out_ref[...] = (secf[...] + of[...]).astype(BF16)

    for src, sem in pending:
        await_bytes(src, sem)
    for p in range(ZN):
        for refs, direct in ((az_s, DIRECT_IN), (fi_s, DIRECT_OUT)):
            for dx in targets(ZORD[p], direct):
                count = TN - 1 if ZORD[p] == 0 and dx == 0 else TN
                await_bytes(seg.at[pl.ds(0, count)], refs.at[dx, p])
    store_mem.wait()


def write_out(*refs):
    ins, outs, sems = refs[:4], refs[4:8], refs[8]
    pairs = [(ins[k], outs[k]) for k in (0, 2, 3)]
    pairs += [(ins[1].at[pl.ds(k, 4)], outs[1].at[pl.ds(k, 4)]) for k in range(0, ROWS, 4)]
    copies = [pltpu.make_async_copy(src, dst, sems.at[k]) for k, (src, dst) in enumerate(pairs)]
    for copy in copies:
        copy.start()
    for copy in copies:
        copy.wait()


def per_device(
    tokens, memory, normalizer, stabilizer, norm_gain, query_weight, key_weight, value_weight, outgate_weight,
    input_gate_weight, forget_gate_weight, forget_bias, memory_gain, proj_weight, ffn_gain, up_weight, down_weight,
):
    hbm = pl.BlockSpec(memory_space=pltpu.HBM)
    anywhere = pl.BlockSpec(memory_space=pl.ANY)
    vmem = pl.BlockSpec(memory_space=pltpu.VMEM)
    dma = pltpu.SemaphoreType.DMA
    outs = (
        jax.ShapeDtypeStruct((ROWS, DB), BF16),
        jax.ShapeDtypeStruct((ROWS, DK, DK), F32),
        jax.ShapeDtypeStruct((ROWS, DK), F32),
        jax.ShapeDtypeStruct((1, ROWS), F32),
    )
    layer_out, memory_new, normalizer_new, stab_new = pl.pallas_call(
        kernel,
        out_shape=outs,
        in_specs=[hbm] * 17,
        out_specs=(vmem, anywhere, vmem, vmem),
        scratch_shapes=[
            pltpu.VMEM((ROWS, D), BF16),
            pltpu.VMEM((ROWS, DK, DK), F32),
            pltpu.VMEM((ROWS, DK), F32),
            pltpu.VMEM((1, ROWS), F32),
            pltpu.VMEM((1, D), F32),
            pltpu.VMEM((D, 4 * DK), BF16),
            pltpu.VMEM((TN, D), BF16),
            pltpu.VMEM((TN, D), BF16),
            pltpu.VMEM((1, TN), F32),
            pltpu.VMEM((1, DK), F32),
            pltpu.VMEM((TN * DK, DB), BF16),
            pltpu.VMEM((1, D), F32),
            pltpu.VMEM((D, FB), BF16),
            pltpu.VMEM((TN, FB, DB), BF16),
            pltpu.VMEM((ROWS, D), BF16),
            pltpu.VMEM((ROWS, DK), F32),
            pltpu.VMEM((2, ROWS, DK), F32),
            pltpu.VMEM((DK, DK), F32),
            pltpu.VMEM((ROWS, TN * DK), BF16),
            pltpu.VMEM((ROWS, DB), F32),
            pltpu.VMEM((TN, SUB, DB), BF16),
            pltpu.VMEM((XN, ZN, TN, SUB, DB), BF16),
            pltpu.VMEM((ROWS, D), F32),
            pltpu.VMEM((ROWS, D), F32),
            pltpu.VMEM((XN, ZN, TN, SUB, DB), BF16),
            pltpu.VMEM((XN - 1, ZN, TN, SUB, DB), BF16),
            pltpu.VMEM((ZN, TN, SUB, DB), F32),
            pltpu.VMEM((ZN, TN, SUB, DB), BF16),
            pltpu.VMEM((XN, ZN, TN, SUB, DB), BF16),
            pltpu.VMEM((ROWS, DB), F32),
            dma((18,)),
            dma((7,)), dma((7,)),
            dma((7,)), dma((7,)),
            dma((7,)), dma((7,)),
            dma((4, 7)), dma((4, 7)),
            dma((XN, ZN)), dma((XN, ZN)),
            dma((XN - 1, ZN)), dma((XN - 1, ZN)),
            dma((XN - 1, ZN)), dma((XN - 1, ZN)),
            dma((XN, ZN)), dma((XN, ZN)),
            pltpu.SemaphoreType.REGULAR((3,)),
            pltpu.SemaphoreType.REGULAR((2,)),
        ],
        compiler_params=pltpu.CompilerParams(
            collective_id=0, has_side_effects=True, vmem_limit_bytes=40 * 1024 * 1024
        ),
        name="layer",
    )(
        *(
            pltpu.with_memory_space_constraint(a, pltpu.HBM)
            for a in (
                tokens,
                memory.reshape(ROWS, DK, DK),
                normalizer.reshape(ROWS, DK),
                stabilizer.T,
                norm_gain.reshape(1, D),
                query_weight, key_weight, value_weight, outgate_weight,
                input_gate_weight.T,
                forget_gate_weight.T,
                forget_bias.reshape(1, TN),
                memory_gain.reshape(1, DK),
                proj_weight,
                ffn_gain.reshape(1, DB),
                up_weight,
                down_weight,
            )
        )
    )
    layer_out, memory_new, normalizer_new, stab_new = pl.pallas_call(
        write_out,
        out_shape=outs,
        in_specs=[anywhere] * 4,
        out_specs=(hbm,) * 4,
        scratch_shapes=[dma((11,))],
        compiler_params=pltpu.CompilerParams(vmem_limit_bytes=4 * 1024 * 1024),
        name="write_out",
    )(layer_out, memory_new, normalizer_new, stab_new)
    return (
        layer_out,
        memory_new.reshape(ROWS, 1, DK, DK),
        normalizer_new.reshape(ROWS, 1, DK),
        stab_new.T,
    )


def solution(mesh):
    placed = (
        P("kv", "tp"),
        P("kv", "tp", None, None),
        P("kv", "tp", None),
        P("kv", "tp"),
        P(),
        P(None, "tp"),
        P(None, "tp"),
        P(None, "tp"),
        P(None, "tp"),
        P(),
        P(),
        P(),
        P("tp"),
        P(None, "tp"),
        P("tp"),
        P("tp", "kv"),
        P("kv", "tp"),
    )
    outs = (P("kv", "tp"), P("kv", "tp", None, None), P("kv", "tp", None), P("kv", "tp"))
    return jax.shard_map(per_device, mesh=mesh, in_specs=placed, out_specs=outs, check_vma=False)
```

```python
import jax
import jax.numpy as jnp
from jax import lax
from jax.experimental import pallas as pl
from jax.experimental.pallas import tpu as pltpu
from jax.sharding import PartitionSpec as P

D = 2048
DK = 128
EPS = 1e-06
XN = 4
ZN = 8
YN = 4
TN = 8
ROWS = 32
DB = D // TN
SUB = ROWS // TN
FB = 256
ZORD = (0, 1, 7, 2, 6, 3, 5, 4)
ZSEND = (0, 2, 6, 3, 5, 4)
NEXT = (1, 7)
DIRECT_IN = (0,)
DIRECT_OUT = (4,)
ORDER = (
    "d", "f2", "f6", "r0", "r1", "f3", "f5", "r2", "r3", "f4", "w",
    "m0", "m17", "m26", "m35", "m4", "z", "s2", "s6", "s3", "s5", "s0",
)
ZPOS = tuple(ZORD.index(o) for o in range(ZN))
HOME = ZPOS[0]
TPO = ((2, 0), (2, 1), (1, 0), (1, 1), (3, 0), (3, 1), (0, 1))
F32 = jnp.float32
BF16 = jnp.bfloat16
MESH = pl.DeviceIdType.MESH


def remote(src, dst, send_sem, recv_sem, kv, tp):
    return pltpu.make_async_remote_copy(
        src_ref=src,
        dst_ref=dst,
        send_sem=send_sem,
        recv_sem=recv_sem,
        device_id={"kv": kv, "tp": tp},
        device_id_type=MESH,
    )


def await_bytes(ref, sem):
    pltpu.make_async_copy(ref, ref, sem).wait()


def kernel(
    tok_h, mem_h, nrm_h, stab_h, ng_h, qw_h, kw_h, vw_h, ow_h, ig_h, fg_h, fb_h, mg_h, pw_h, gain_h, up_h, dn_h,
    out_ref, memn_h, nrmn_ref, stabn_ref,
    tk, mem, nrm, stab, ng, qkvo, ig, fg, fb, mg, pw, gains, upb, dnb,
    qf, colrow, colmat, mx, secf, seg, xbuf, xs, os, rsx_s, rsx_r, own, own_row, rows_z, zs, fin, of,
    lsem, tok_s, tok_r, gain_s, gain_r, mix_s, mix_r, w_s, w_r, az_s, az_r, xf_s, xf_r, rx_s, rx_r, fi_s, fi_r, gz_s, gz_r, hz_s, hz_r,
    zready, xready,
):
    kv = lax.axis_index("kv")
    t = lax.axis_index("tp")
    z, x = kv // XN, kv % XN
    y, c = t // 2, t % 2

    def zx(dz, dx):
        return ((z + dz) % ZN) * XN + (x + dx) % XN

    def tp_at(dy, dc):
        return ((y + dy) % YN) * 2 + (c + dc) % 2

    pending = []

    def send(src, dst, ssem, rsem, kv_to, tp_to):
        remote(src, dst, ssem, rsem, kv_to, tp_to).start()
        pending.append((src, ssem))

    lane_t = pl.ds(pl.multiple_of(t * DB, DB), DB)
    lane_h = pl.ds(pl.multiple_of(t * DK, DK), DK)
    row_t = lane_t

    loads = {}

    def load(name, src, dst):
        k = len(loads)
        loads[name] = pltpu.make_async_copy(src, dst, lsem.at[k])
        loads[name].start()

    load("tok", tok_h, tk.at[:, lane_t])
    load("gain", gain_h, gains.at[:, lane_t])
    load("up", up_h, upb.at[row_t])
    load("dn", dn_h, dnb.at[t])
    load("ng", ng_h, ng)
    for k, (name, w) in enumerate((("q", qw_h), ("k", kw_h), ("v", vw_h), ("o", ow_h))):
        load(name, w, qkvo.at[:, DK * k : DK * (k + 1)])
    load("ig", ig_h, ig)
    load("fg", fg_h, fg)
    load("fb", fb_h, fb)
    load("stab", stab_h, stab)
    load("nrm", nrm_h, nrm)
    load("mem", mem_h, mem)
    load("mg", mg_h, mg)
    load("pw", pw_h, pw)

    def tell(sem, kv_to, tp_to):
        pl.semaphore_signal(sem, inc=1, device_id={"kv": kv_to, "tp": tp_to}, device_id_type=MESH)

    barrier = pltpu.get_barrier_semaphore()
    for dy, dc in TPO:
        tell(barrier, kv, tp_at(dy, dc))
    for step in (1, -1):
        tell(barrier, zx(0, step), t)
        tell(barrier, zx(step, 0), t)
    pl.semaphore_wait(barrier, 7 + 4)
    for step in (1, -1):
        tell(xready.at[0], zx(0, step), t)
        tell(zready.at[0], zx(step, 0), t)

    loads["tok"].wait()
    for k, (dy, dc) in enumerate(TPO):
        send(tk.at[:, lane_t], tk.at[:, lane_t], tok_s.at[k], tok_r.at[k], kv, tp_at(dy, dc))
    loads["gain"].wait()
    for k, (dy, dc) in enumerate(TPO):
        send(gains.at[:, lane_t], gains.at[:, lane_t], gain_s.at[k], gain_r.at[k], kv, tp_at(dy, dc))

    def w_slot(m, dy, dc):
        s = tp_at(dy, dc)
        if m < 2:
            return upb.at[pl.ds(pl.multiple_of(s * DB + DB // 2 * m, DB // 2), DB // 2)]
        return dnb.at[s, pl.ds(FB // 2 * (m - 2), FB // 2)]

    def send_weights(m):
        slot = w_slot(m, 0, 0)
        for k, (dy, dc) in ((0, (1, 0)), (1, (3, 0)), (3, (0, 1))):
            send(slot, slot, w_s.at[m, k], w_r.at[m, k], kv, tp_at(dy, dc))

    loads["up"].wait()
    send_weights(0)
    send_weights(1)

    pl.semaphore_wait(xready.at[0], 2)
    pl.semaphore_wait(zready.at[0], 2)
    for step in (2, -2):
        tell(zready.at[1], zx(step, 0), t)

    def chip_slice(dy, width):
        return pl.ds(pl.multiple_of(((y - dy) % YN) * 2 * width, 2 * width), 2 * width)

    def await_chip(dy, recv):
        for k, (other, dc) in enumerate(TPO):
            if other == dy:
                await_bytes(recv[0](tp_at(-dy, -dc)), recv[1].at[k])

    for name in ("ng", "q", "k", "v", "o", "ig", "fg", "fb", "stab", "nrm"):
        loads[name].wait()
    contract = (((1,), (1,)), ((), ()))
    square_sum = jnp.zeros((ROWS, 1), F32)
    proj4 = jnp.zeros((ROWS, 4 * DK), F32)
    all_in = jnp.zeros((ROWS, TN), F32)
    all_forget = jnp.zeros((ROWS, TN), F32)
    for dy in (0, 1, 3, 2):
        if dy == 1:
            pl.semaphore_wait(zready.at[1], 2)
            for step in (3, -3, 4):
                tell(zready.at[2], zx(step, 0), t)
        await_chip(dy, (lambda s: tk.at[:, pl.ds(pl.multiple_of(s * DB, DB), DB)], tok_r))
        cols = chip_slice(dy, DB)
        rows = tk[:, cols].astype(F32)
        square_sum += jnp.sum(rows * rows, axis=-1, keepdims=True)
        gained = (rows * ng[:, cols]).astype(BF16)
        proj4 += jnp.dot(gained, qkvo[cols, :], preferred_element_type=F32)
        all_in += lax.dot_general(gained, ig[:, cols], contract, preferred_element_type=F32)
        all_forget += lax.dot_general(gained, fg[:, cols], contract, preferred_element_type=F32)
    scale_one = lax.rsqrt(square_sum * (1.0 / D) + EPS)
    proj4 = (proj4 * scale_one).astype(BF16).astype(F32)
    query = proj4[:, :DK]
    keys = proj4[:, DK : 2 * DK] * DK ** (-0.5)
    values = proj4[:, 2 * DK : 3 * DK]
    gate_out = proj4[:, 3 * DK :]
    qf[...] = query

    all_in = all_in * scale_one
    all_forget = all_forget * scale_one + fb[...]
    head = lax.broadcasted_iota(jnp.int32, (ROWS, TN), 1) == t
    input_log = jnp.sum(jnp.where(head, all_in, 0.0), axis=1, keepdims=True)
    raw = jnp.sum(jnp.where(head, all_forget, 0.0), axis=1, keepdims=True)
    forget_log = jnp.minimum(raw, 0.0) - jnp.log1p(jnp.exp(-jnp.abs(raw)))
    diag = lax.broadcasted_iota(jnp.int32, (ROWS, ROWS), 0) == lax.broadcasted_iota(jnp.int32, (ROWS, ROWS), 1)
    stab_col = jnp.sum(jnp.where(diag, jnp.broadcast_to(stab[...], (ROWS, ROWS)), 0.0), axis=1, keepdims=True)
    stab_new = jnp.maximum(forget_log + stab_col, input_log)
    keep = jnp.exp(forget_log + stab_col - stab_new)
    admit = jnp.exp(input_log - stab_new)
    normalizer_new = keep * nrm[...] + admit * keys
    denom = jnp.sum(normalizer_new * query, axis=1, keepdims=True)
    key_query = jnp.sum(keys * query, axis=1, keepdims=True)

    loads["mem"].wait()
    lane = lax.broadcasted_iota(jnp.int32, (DK, DK), 1)

    def read_memory(b, acc):
        part = jnp.sum(mem[b] * qf[pl.ds(b, 1), :], axis=1, keepdims=True)
        return jnp.where(lane == b, part, acc)

    read = lax.fori_loop(0, ROWS, read_memory, jnp.zeros((DK, DK), F32), unroll=ROWS)
    memory_query = read.T[:ROWS, :]
    numer = keep * memory_query + (admit * key_query) * values
    cell = numer / jnp.maximum(jnp.abs(denom), 1.0)
    loads["mg"].wait()
    mx[:, lane_h] = (cell * mg[...] * jax.nn.sigmoid(gate_out)).astype(BF16)
    for k, (dy, dc) in enumerate(TPO):
        send(mx.at[:, lane_h], mx.at[:, lane_h], mix_s.at[k], mix_r.at[k], kv, tp_at(dy, dc))

    loads["dn"].wait()
    send_weights(2)
    send_weights(3)
    nrmn_ref[...] = normalizer_new
    stabn_ref[...] = jnp.sum(
        jnp.where(diag, jnp.broadcast_to(stab_new, (ROWS, ROWS)), 0.0), axis=0, keepdims=True
    )
    colrow[0] = jnp.broadcast_to(keep, (ROWS, DK))
    colrow[1] = keys
    colmat[:ROWS, :] = admit * values
    colmat[ROWS:, :] = jnp.zeros((DK - ROWS, DK), F32)
    admitted = colmat[...].T

    def write_memory(b, carry):
        column = jnp.sum(jnp.where(lane == b, admitted, 0.0), axis=1, keepdims=True)
        mem[b] = colrow[0, pl.ds(b, 1), :] * mem[b] + column * colrow[1, pl.ds(b, 1), :]
        return carry

    lax.fori_loop(0, ROWS, write_memory, 0, unroll=ROWS)
    store_mem = pltpu.make_async_copy(mem, memn_h, lsem.at[len(loads)])
    store_mem.start()

    pl.semaphore_wait(zready.at[2], 3)
    for dx in range(1, XN):
        tell(xready.at[1], zx(0, dx), t)

    def relay(m, k, dy, forward):
        slot = w_slot(m, dy, 0)
        await_bytes(slot, w_r.at[m, k])
        if forward is not None:
            send(slot, slot, w_s.at[m, 2], w_r.at[m, 2], kv, tp_at(forward, 0))
        send(slot, slot, w_s.at[m, 4 + k], w_r.at[m, 4 + k], kv, tp_at(0, 1))

    loads["pw"].wait()
    projected = jnp.zeros((ROWS, DB), F32)
    for dy in (0, 1, 3, 2):
        await_chip(dy, (lambda s: mx.at[:, pl.ds(pl.multiple_of(s * DK, DK), DK)], mix_r))
        cols = chip_slice(dy, DK)
        projected += jnp.dot(mx[:, cols], pw[cols, :], preferred_element_type=F32)
    second = (tk[:, lane_t].astype(F32) + projected).astype(BF16).astype(F32)
    secf[...] = second
    for s in range(TN):
        seg[s] = secf[SUB * s : SUB * (s + 1), :].astype(BF16)

    def scatter(dz, dx, src, dst, ssem, rsem):
        there = ZPOS[(-dz) % ZN]
        slot = (-dx) % XN
        for dy, dc in TPO + ((0, 0),):
            s = tp_at(dy, dc)
            if dz == 0 and dx == 0 and (dy, dc) == (0, 0):
                pltpu.make_async_copy(src.at[s], dst.at[slot, there, t], rsem.at[slot, there]).start()
            else:
                remote(
                    src.at[s], dst.at[slot, there, t], ssem.at[dx, ZPOS[dz]], rsem.at[slot, there], zx(dz, dx), s
                ).start()

    def targets(dz, direct):
        if dz in NEXT:
            return ()
        return range(XN) if dz in direct else (0,)

    pl.semaphore_wait(xready.at[1], XN - 1)
    for dz in ZSEND:
        for dx in targets(dz, DIRECT_IN):
            scatter(dz, dx, seg, xbuf, az_s, az_r)

    relay(0, 0, 3, 1)
    relay(1, 1, 1, 3)
    relay(0, 1, 1, None)
    relay(1, 0, 3, None)
    relay(2, 1, 1, 3)
    relay(3, 0, 3, 1)
    relay(2, 0, 3, None)
    relay(3, 1, 1, None)

    def forward(dz):
        p = ZPOS[dz]
        await_bytes(xbuf.at[0, p], az_r.at[0, p])
        for dx in range(1, XN):
            send(
                xbuf.at[0, p], xbuf.at[(-dx) % XN, p],
                xf_s.at[dx - 1, p], xf_r.at[(-dx) % XN - 1, p], zx(0, dx), t,
            )

    def spread_row():
        for dx in range(XN):
            await_bytes(xbuf.at[dx, HOME], az_r.at[dx, HOME])
        for k, dz in enumerate(NEXT):
            there = ZPOS[(-dz) % ZN]
            send(xbuf.at[:, HOME], xbuf.at[:, there], gz_s.at[k], gz_r.at[there - 1], zx(dz, 0), t)

    def rest_of_weights():
        for k, (dy, dc) in enumerate(TPO):
            s = tp_at(-dy, -dc)
            await_bytes(gains.at[:, pl.ds(pl.multiple_of(s * DB, DB), DB)], gain_r.at[k])
        for m in range(4):
            for k, dy in ((3, 0), (4, 3), (5, 1), (6, 2)):
                await_bytes(w_slot(m, dy, 1), w_r.at[m, k])

    def send_along_x(p):
        for dx in range(1, XN):
            send(
                rsx_s.at[dx, p], rsx_r.at[(-dx) % XN - 1, p],
                rx_s.at[dx - 1, p], rx_r.at[(-dx) % XN - 1, p], zx(0, dx), t,
            )

    def mixer(group):
        blocks = [(dx, ZPOS[dz]) for dx in range(XN) for dz in group]
        count = SUB * len(blocks)
        for dz in group:
            p = ZPOS[dz]
            if dz in NEXT:
                await_bytes(xbuf.at[:, p], gz_r.at[p - 1])
            elif dz != 0:
                for dx in range(1, XN):
                    await_bytes(xbuf.at[dx, p], xf_r.at[dx - 1, p])
        for i, (dx, p) in enumerate(blocks):
            block = xbuf[dx, p].astype(F32)
            for j in range(TN):
                xs[SUB * i : SUB * (i + 1), DB * j : DB * (j + 1)] = block[j]
        sec = xs[:count, :]
        scale_two = lax.rsqrt(jnp.sum(sec * sec, axis=-1, keepdims=True) * (1.0 / D) + EPS)
        scaled = (sec * gains[...]).astype(BF16)
        preact = jnp.dot(scaled, upb[...], preferred_element_type=F32)
        hidden = jnp.square(jnp.maximum(preact * scale_two, 0.0)).astype(BF16)
        for j in range(TN):
            os[:count, DB * j : DB * (j + 1)] = jnp.dot(hidden, dnb[j], preferred_element_type=F32)
        for i, (dx, p) in enumerate(blocks):
            for j in range(TN):
                block = os[SUB * i : SUB * (i + 1), DB * j : DB * (j + 1)]
                if p == HOME:
                    own_row[dx, j] = block
                elif dx == 0 and ZORD[p] not in DIRECT_OUT + NEXT:
                    own[p, j] = block
                else:
                    rsx_s[dx, p, j] = block.astype(BF16)
        for dz in group:
            p = ZPOS[dz]
            if dz in DIRECT_OUT:
                for dx in range(XN):
                    scatter(dz, dx, rsx_s.at[dx, p], fin, fi_s, fi_r)
            elif dz in NEXT:
                there = ZPOS[(-dz) % ZN] - 1
                send(rsx_s.at[:, p], rows_z.at[there], hz_s.at[p - 1], hz_r.at[there], zx(dz, 0), t)
            elif dz != 0:
                send_along_x(p)

    def sum_z():
        for k in range(2):
            await_bytes(rows_z.at[k], hz_r.at[k])
        for dx in range(XN):
            total = own_row[dx] + rows_z[0, dx].astype(F32) + rows_z[1, dx].astype(F32)
            if dx == 0:
                own[HOME] = total
            else:
                rsx_s[dx, HOME] = total.astype(BF16)
        send_along_x(HOME)

    def sum_x(p):
        for dx in range(1, XN):
            await_bytes(rsx_r.at[dx - 1, p], rx_r.at[dx - 1, p])
        total = own[p]
        for dx in range(1, XN):
            total += rsx_r[dx - 1, p].astype(F32)
        zs[p] = total.astype(BF16)
        scatter(ZORD[p], 0, zs.at[p], fin, fi_s, fi_r)

    for step in ORDER:
        group = [int(digit) for digit in step[1:]]
        if step == "w":
            rest_of_weights()
        elif step == "d":
            spread_row()
        elif step == "z":
            sum_z()
        elif step[0] == "r":
            relay(group[0], 2, 2, None)
        elif step[0] == "f":
            forward(group[0])
        elif step[0] == "m":
            mixer(group)
        else:
            sum_x(ZPOS[group[0]])

    total = jnp.zeros((TN, SUB, DB), F32)
    for p in range(ZN):
        for dx in targets(ZORD[p], DIRECT_OUT):
            await_bytes(fin.at[dx, p], fi_r.at[dx, p])
            total += fin[dx, p].astype(F32)
    for s in range(TN):
        of[SUB * s : SUB * (s + 1), :] = total[s]
    out_ref[...] = (secf[...] + of[...]).astype(BF16)

    for src, sem in pending:
        await_bytes(src, sem)
    for p in range(ZN):
        for refs, direct in ((az_s, DIRECT_IN), (fi_s, DIRECT_OUT)):
            for dx in targets(ZORD[p], direct):
                count = TN - 1 if ZORD[p] == 0 and dx == 0 else TN
                await_bytes(seg.at[pl.ds(0, count)], refs.at[dx, p])
    store_mem.wait()


def write_out(*refs):
    ins, outs, sems = refs[:4], refs[4:8], refs[8]
    pairs = [(ins[k], outs[k]) for k in (0, 2, 3)]
    pairs += [(ins[1].at[pl.ds(k, 4)], outs[1].at[pl.ds(k, 4)]) for k in range(0, ROWS, 4)]
    copies = [pltpu.make_async_copy(src, dst, sems.at[k]) for k, (src, dst) in enumerate(pairs)]
    for copy in copies:
        copy.start()
    for copy in copies:
        copy.wait()


def per_device(
    tokens, memory, normalizer, stabilizer, norm_gain, query_weight, key_weight, value_weight, outgate_weight,
    input_gate_weight, forget_gate_weight, forget_bias, memory_gain, proj_weight, ffn_gain, up_weight, down_weight,
):
    hbm = pl.BlockSpec(memory_space=pltpu.HBM)
    anywhere = pl.BlockSpec(memory_space=pl.ANY)
    vmem = pl.BlockSpec(memory_space=pltpu.VMEM)
    dma = pltpu.SemaphoreType.DMA
    outs = (
        jax.ShapeDtypeStruct((ROWS, DB), BF16),
        jax.ShapeDtypeStruct((ROWS, DK, DK), F32),
        jax.ShapeDtypeStruct((ROWS, DK), F32),
        jax.ShapeDtypeStruct((1, ROWS), F32),
    )
    layer_out, memory_new, normalizer_new, stab_new = pl.pallas_call(
        kernel,
        out_shape=outs,
        in_specs=[hbm] * 17,
        out_specs=(vmem, anywhere, vmem, vmem),
        scratch_shapes=[
            pltpu.VMEM((ROWS, D), BF16),
            pltpu.VMEM((ROWS, DK, DK), F32),
            pltpu.VMEM((ROWS, DK), F32),
            pltpu.VMEM((1, ROWS), F32),
            pltpu.VMEM((1, D), F32),
            pltpu.VMEM((D, 4 * DK), BF16),
            pltpu.VMEM((TN, D), BF16),
            pltpu.VMEM((TN, D), BF16),
            pltpu.VMEM((1, TN), F32),
            pltpu.VMEM((1, DK), F32),
            pltpu.VMEM((TN * DK, DB), BF16),
            pltpu.VMEM((1, D), F32),
            pltpu.VMEM((D, FB), BF16),
            pltpu.VMEM((TN, FB, DB), BF16),
            pltpu.VMEM((ROWS, DK), F32),
            pltpu.VMEM((2, ROWS, DK), F32),
            pltpu.VMEM((DK, DK), F32),
            pltpu.VMEM((ROWS, TN * DK), BF16),
            pltpu.VMEM((ROWS, DB), F32),
            pltpu.VMEM((TN, SUB, DB), BF16),
            pltpu.VMEM((XN, ZN, TN, SUB, DB), BF16),
            pltpu.VMEM((ROWS, D), F32),
            pltpu.VMEM((ROWS, D), F32),
            pltpu.VMEM((XN, ZN, TN, SUB, DB), BF16),
            pltpu.VMEM((XN - 1, ZN, TN, SUB, DB), BF16),
            pltpu.VMEM((ZN, TN, SUB, DB), F32),
            pltpu.VMEM((XN, TN, SUB, DB), F32),
            pltpu.VMEM((2, XN, TN, SUB, DB), BF16),
            pltpu.VMEM((ZN, TN, SUB, DB), BF16),
            pltpu.VMEM((XN, ZN, TN, SUB, DB), BF16),
            pltpu.VMEM((ROWS, DB), F32),
            dma((18,)),
            dma((7,)), dma((7,)),
            dma((7,)), dma((7,)),
            dma((7,)), dma((7,)),
            dma((4, 7)), dma((4, 7)),
            dma((XN, ZN)), dma((XN, ZN)),
            dma((XN - 1, ZN)), dma((XN - 1, ZN)),
            dma((XN - 1, ZN)), dma((XN - 1, ZN)),
            dma((XN, ZN)), dma((XN, ZN)),
            dma((2,)), dma((2,)),
            dma((2,)), dma((2,)),
            pltpu.SemaphoreType.REGULAR((3,)),
            pltpu.SemaphoreType.REGULAR((2,)),
        ],
        compiler_params=pltpu.CompilerParams(
            collective_id=0, has_side_effects=True, vmem_limit_bytes=40 * 1024 * 1024
        ),
        name="layer",
    )(
        *(
            pltpu.with_memory_space_constraint(a, pltpu.HBM)
            for a in (
                tokens,
                memory.reshape(ROWS, DK, DK),
                normalizer.reshape(ROWS, DK),
                stabilizer.T,
                norm_gain.reshape(1, D),
                query_weight, key_weight, value_weight, outgate_weight,
                input_gate_weight.T,
                forget_gate_weight.T,
                forget_bias.reshape(1, TN),
                memory_gain.reshape(1, DK),
                proj_weight,
                ffn_gain.reshape(1, DB),
                up_weight,
                down_weight,
            )
        )
    )
    layer_out, memory_new, normalizer_new, stab_new = pl.pallas_call(
        write_out,
        out_shape=outs,
        in_specs=[anywhere] * 4,
        out_specs=(hbm,) * 4,
        scratch_shapes=[dma((11,))],
        compiler_params=pltpu.CompilerParams(vmem_limit_bytes=4 * 1024 * 1024),
        name="write_out",
    )(layer_out, memory_new, normalizer_new, stab_new)
    return (
        layer_out,
        memory_new.reshape(ROWS, 1, DK, DK),
        normalizer_new.reshape(ROWS, 1, DK),
        stab_new.T,
    )


def solution(mesh):
    placed = (
        P("kv", "tp"),
        P("kv", "tp", None, None),
        P("kv", "tp", None),
        P("kv", "tp"),
        P(),
        P(None, "tp"),
        P(None, "tp"),
        P(None, "tp"),
        P(None, "tp"),
        P(),
        P(),
        P(),
        P("tp"),
        P(None, "tp"),
        P("tp"),
        P("tp", "kv"),
        P("kv", "tp"),
    )
    outs = (P("kv", "tp"), P("kv", "tp", None, None), P("kv", "tp", None), P("kv", "tp"))
    return jax.shard_map(per_device, mesh=mesh, in_specs=placed, out_specs=outs, check_vma=False)
```

```python
import jax
import jax.numpy as jnp
from jax import lax
from jax.experimental import pallas as pl
from jax.experimental.pallas import tpu as pltpu
from jax.sharding import PartitionSpec as P

D = 2048
DK = 128
EPS = 1e-06
XN = 4
ZN = 8
YN = 4
TN = 8
ROWS = 32
DB = D // TN
SUB = ROWS // TN
FB = 256
ZORD = (0, 1, 7, 2, 6, 3, 5, 4)
ZSEND = (2, 6, 3, 5, 0, 4)
NEXT = (1, 7)
DIRECT_IN = (0,)
DIRECT_OUT = (4,)
ORDER = (
    "d", "f2", "f6", "r0", "r1", "f3", "f5", "r2", "r3", "f4", "w", "m0", "m17", "m26", "m35", "m4", "z", "s2", "s6", "s3", "s5", "s0",
)
ZPOS = tuple(ZORD.index(o) for o in range(ZN))
HOME = ZPOS[0]
TPO = ((2, 0), (2, 1), (1, 0), (1, 1), (3, 0), (3, 1), (0, 1))
F32 = jnp.float32
BF16 = jnp.bfloat16
MESH = pl.DeviceIdType.MESH


def remote(src, dst, send_sem, recv_sem, kv, tp):
    return pltpu.make_async_remote_copy(
        src_ref=src,
        dst_ref=dst,
        send_sem=send_sem,
        recv_sem=recv_sem,
        device_id={"kv": kv, "tp": tp},
        device_id_type=MESH,
    )


def await_bytes(ref, sem):
    pltpu.make_async_copy(ref, ref, sem).wait()


def kernel(
    tok_h, mem_h, nrm_h, stab_h, ng_h, qw_h, kw_h, vw_h, ow_h, ig_h, fg_h, fb_h, mg_h, pw_h, gain_h, up_h, dn_h,
    out_ref, memn_h, nrmn_ref, stabn_ref,
    tk, mem, nrm, stab, ng, qkvo, ig, fg, fb, mg, pw, gains, upb, dnb,
    qf, colrow, colmat, mx, secf, seg, xbuf, xs, os, rsx_s, rsx_r, own, own_row, rows_z, zs, fin, of,
    lsem, tok_s, tok_r, gain_s, gain_r, mix_s, mix_r, w_s, w_r, az_s, az_r, xf_s, xf_r, rx_s, rx_r, fi_s, fi_r, gz_s, gz_r, hz_s, hz_r,
    zready, xready,
):
    kv = lax.axis_index("kv")
    t = lax.axis_index("tp")
    z, x = kv // XN, kv % XN
    y, c = t // 2, t % 2

    def zx(dz, dx):
        return ((z + dz) % ZN) * XN + (x + dx) % XN

    def tp_at(dy, dc):
        return ((y + dy) % YN) * 2 + (c + dc) % 2

    pending = []

    def send(src, dst, ssem, rsem, kv_to, tp_to):
        remote(src, dst, ssem, rsem, kv_to, tp_to).start()
        pending.append((src, ssem))

    lane_t = pl.ds(pl.multiple_of(t * DB, DB), DB)
    lane_h = pl.ds(pl.multiple_of(t * DK, DK), DK)
    row_t = lane_t

    loads = {}

    def load(name, src, dst):
        k = len(loads)
        loads[name] = pltpu.make_async_copy(src, dst, lsem.at[k])
        loads[name].start()

    load("tok", tok_h, tk.at[:, lane_t])
    load("gain", gain_h, gains.at[:, lane_t])
    load("up", up_h, upb.at[row_t])
    load("dn", dn_h, dnb.at[t])
    load("ng", ng_h, ng)
    for k, (name, w) in enumerate((("q", qw_h), ("k", kw_h), ("v", vw_h), ("o", ow_h))):
        load(name, w, qkvo.at[:, DK * k : DK * (k + 1)])
    load("ig", ig_h, ig)
    load("fg", fg_h, fg)
    load("fb", fb_h, fb)
    load("stab", stab_h, stab)
    load("nrm", nrm_h, nrm)
    load("mem", mem_h, mem)
    load("mg", mg_h, mg)
    load("pw", pw_h, pw)

    def tell(sem, kv_to, tp_to):
        pl.semaphore_signal(sem, inc=1, device_id={"kv": kv_to, "tp": tp_to}, device_id_type=MESH)

    barrier = pltpu.get_barrier_semaphore()
    for dy, dc in TPO:
        tell(barrier, kv, tp_at(dy, dc))
    for step in (1, -1):
        tell(barrier, zx(0, step), t)
        tell(barrier, zx(step, 0), t)
    pl.semaphore_wait(barrier, 7 + 4)
    for step in (1, -1):
        tell(xready.at[0], zx(0, step), t)
        tell(zready.at[0], zx(step, 0), t)

    loads["tok"].wait()
    for k, (dy, dc) in enumerate(TPO):
        send(tk.at[:, lane_t], tk.at[:, lane_t], tok_s.at[k], tok_r.at[k], kv, tp_at(dy, dc))
    loads["gain"].wait()
    for k, (dy, dc) in enumerate(TPO):
        send(gains.at[:, lane_t], gains.at[:, lane_t], gain_s.at[k], gain_r.at[k], kv, tp_at(dy, dc))

    def w_slot(m, dy, dc):
        s = tp_at(dy, dc)
        if m < 2:
            return upb.at[pl.ds(pl.multiple_of(s * DB + DB // 2 * m, DB // 2), DB // 2)]
        return dnb.at[s, pl.ds(FB // 2 * (m - 2), FB // 2)]

    def send_weights(m):
        slot = w_slot(m, 0, 0)
        for k, (dy, dc) in ((0, (1, 0)), (1, (3, 0)), (3, (0, 1))):
            send(slot, slot, w_s.at[m, k], w_r.at[m, k], kv, tp_at(dy, dc))

    loads["up"].wait()
    send_weights(0)
    send_weights(1)

    pl.semaphore_wait(xready.at[0], 2)
    pl.semaphore_wait(zready.at[0], 2)
    for step in (2, -2):
        tell(zready.at[1], zx(step, 0), t)

    def chip_slice(dy, width):
        return pl.ds(pl.multiple_of(((y - dy) % YN) * 2 * width, 2 * width), 2 * width)

    def await_chip(dy, recv):
        for k, (other, dc) in enumerate(TPO):
            if other == dy:
                await_bytes(recv[0](tp_at(-dy, -dc)), recv[1].at[k])

    for name in ("ng", "q", "k", "v", "o", "ig", "fg", "fb", "stab", "nrm"):
        loads[name].wait()
    contract = (((1,), (1,)), ((), ()))
    square_sum = jnp.zeros((ROWS, 1), F32)
    proj4 = jnp.zeros((ROWS, 4 * DK), F32)
    all_in = jnp.zeros((ROWS, TN), F32)
    all_forget = jnp.zeros((ROWS, TN), F32)
    for dy in (0, 1, 3, 2):
        if dy == 1:
            pl.semaphore_wait(zready.at[1], 2)
            for step in (3, -3, 4):
                tell(zready.at[2], zx(step, 0), t)
        await_chip(dy, (lambda s: tk.at[:, pl.ds(pl.multiple_of(s * DB, DB), DB)], tok_r))
        cols = chip_slice(dy, DB)
        rows = tk[:, cols].astype(F32)
        square_sum += jnp.sum(rows * rows, axis=-1, keepdims=True)
        gained = (rows * ng[:, cols]).astype(BF16)
        proj4 += jnp.dot(gained, qkvo[cols, :], preferred_element_type=F32)
        all_in += lax.dot_general(gained, ig[:, cols], contract, preferred_element_type=F32)
        all_forget += lax.dot_general(gained, fg[:, cols], contract, preferred_element_type=F32)
    scale_one = lax.rsqrt(square_sum * (1.0 / D) + EPS)
    proj4 = (proj4 * scale_one).astype(BF16).astype(F32)
    query = proj4[:, :DK]
    keys = proj4[:, DK : 2 * DK] * DK ** (-0.5)
    values = proj4[:, 2 * DK : 3 * DK]
    gate_out = proj4[:, 3 * DK :]
    qf[...] = query

    all_in = all_in * scale_one
    all_forget = all_forget * scale_one + fb[...]
    head = lax.broadcasted_iota(jnp.int32, (ROWS, TN), 1) == t
    input_log = jnp.sum(jnp.where(head, all_in, 0.0), axis=1, keepdims=True)
    raw = jnp.sum(jnp.where(head, all_forget, 0.0), axis=1, keepdims=True)
    forget_log = jnp.minimum(raw, 0.0) - jnp.log1p(jnp.exp(-jnp.abs(raw)))
    diag = lax.broadcasted_iota(jnp.int32, (ROWS, ROWS), 0) == lax.broadcasted_iota(jnp.int32, (ROWS, ROWS), 1)
    stab_col = jnp.sum(jnp.where(diag, jnp.broadcast_to(stab[...], (ROWS, ROWS)), 0.0), axis=1, keepdims=True)
    stab_new = jnp.maximum(forget_log + stab_col, input_log)
    keep = jnp.exp(forget_log + stab_col - stab_new)
    admit = jnp.exp(input_log - stab_new)
    normalizer_new = keep * nrm[...] + admit * keys
    denom = jnp.sum(normalizer_new * query, axis=1, keepdims=True)
    key_query = jnp.sum(keys * query, axis=1, keepdims=True)

    loads["mem"].wait()
    lane = lax.broadcasted_iota(jnp.int32, (DK, DK), 1)

    def read_memory(b, acc):
        part = jnp.sum(mem[b] * qf[pl.ds(b, 1), :], axis=1, keepdims=True)
        return jnp.where(lane == b, part, acc)

    read = lax.fori_loop(0, ROWS, read_memory, jnp.zeros((DK, DK), F32), unroll=ROWS)
    memory_query = read.T[:ROWS, :]
    numer = keep * memory_query + (admit * key_query) * values
    cell = numer / jnp.maximum(jnp.abs(denom), 1.0)
    loads["mg"].wait()
    mx[:, lane_h] = (cell * mg[...] * jax.nn.sigmoid(gate_out)).astype(BF16)
    for k, (dy, dc) in enumerate(TPO):
        send(mx.at[:, lane_h], mx.at[:, lane_h], mix_s.at[k], mix_r.at[k], kv, tp_at(dy, dc))

    loads["dn"].wait()
    send_weights(2)
    send_weights(3)
    nrmn_ref[...] = normalizer_new
    stabn_ref[...] = jnp.sum(
        jnp.where(diag, jnp.broadcast_to(stab_new, (ROWS, ROWS)), 0.0), axis=0, keepdims=True
    )
    colrow[0] = jnp.broadcast_to(keep, (ROWS, DK))
    colrow[1] = keys
    colmat[:ROWS, :] = admit * values
    colmat[ROWS:, :] = jnp.zeros((DK - ROWS, DK), F32)
    admitted = colmat[...].T

    def write_memory(b, carry):
        column = jnp.sum(jnp.where(lane == b, admitted, 0.0), axis=1, keepdims=True)
        mem[b] = colrow[0, pl.ds(b, 1), :] * mem[b] + column * colrow[1, pl.ds(b, 1), :]
        return carry

    lax.fori_loop(0, ROWS, write_memory, 0, unroll=ROWS)
    store_mem = pltpu.make_async_copy(mem, memn_h, lsem.at[len(loads)])
    store_mem.start()

    pl.semaphore_wait(zready.at[2], 3)
    for dx in range(1, XN):
        tell(xready.at[1], zx(0, dx), t)

    def relay(m, k, dy, forward):
        slot = w_slot(m, dy, 0)
        await_bytes(slot, w_r.at[m, k])
        if forward is not None:
            send(slot, slot, w_s.at[m, 2], w_r.at[m, 2], kv, tp_at(forward, 0))
        send(slot, slot, w_s.at[m, 4 + k], w_r.at[m, 4 + k], kv, tp_at(0, 1))

    loads["pw"].wait()
    projected = jnp.zeros((ROWS, DB), F32)
    for dy in (0, 1, 3, 2):
        await_chip(dy, (lambda s: mx.at[:, pl.ds(pl.multiple_of(s * DK, DK), DK)], mix_r))
        cols = chip_slice(dy, DK)
        projected += jnp.dot(mx[:, cols], pw[cols, :], preferred_element_type=F32)
    second = (tk[:, lane_t].astype(F32) + projected).astype(BF16).astype(F32)
    secf[...] = second
    for s in range(TN):
        seg[s] = secf[SUB * s : SUB * (s + 1), :].astype(BF16)

    def scatter(dz, dx, src, dst, ssem, rsem):
        there = ZPOS[(-dz) % ZN]
        slot = (-dx) % XN
        for dy, dc in TPO + ((0, 0),):
            s = tp_at(dy, dc)
            if dz == 0 and dx == 0 and (dy, dc) == (0, 0):
                pltpu.make_async_copy(src.at[s], dst.at[slot, there, t], rsem.at[slot, there]).start()
            else:
                remote(
                    src.at[s], dst.at[slot, there, t], ssem.at[dx, ZPOS[dz]], rsem.at[slot, there], zx(dz, dx), s
                ).start()

    def targets(dz, direct):
        if dz in NEXT:
            return ()
        return (2, 1, 3, 0) if dz in direct else (0,)

    pl.semaphore_wait(xready.at[1], XN - 1)
    for dz in ZSEND:
        for dx in targets(dz, DIRECT_IN):
            scatter(dz, dx, seg, xbuf, az_s, az_r)

    relay(0, 0, 3, 1)
    relay(1, 1, 1, 3)
    relay(0, 1, 1, None)
    relay(1, 0, 3, None)
    relay(2, 1, 1, 3)
    relay(3, 0, 3, 1)
    relay(2, 0, 3, None)
    relay(3, 1, 1, None)

    def forward(dz):
        p = ZPOS[dz]
        await_bytes(xbuf.at[0, p], az_r.at[0, p])
        for dx in (2, 1, 3):
            send(
                xbuf.at[0, p], xbuf.at[(-dx) % XN, p],
                xf_s.at[dx - 1, p], xf_r.at[(-dx) % XN - 1, p], zx(0, dx), t,
            )

    def spread_row():
        for dx in range(XN):
            await_bytes(xbuf.at[dx, HOME], az_r.at[dx, HOME])
        for k, dz in enumerate(NEXT):
            there = ZPOS[(-dz) % ZN]
            send(xbuf.at[:, HOME], xbuf.at[:, there], gz_s.at[k], gz_r.at[there - 1], zx(dz, 0), t)

    def rest_of_weights():
        for k, (dy, dc) in enumerate(TPO):
            s = tp_at(-dy, -dc)
            await_bytes(gains.at[:, pl.ds(pl.multiple_of(s * DB, DB), DB)], gain_r.at[k])
        for m in range(4):
            for k, dy in ((3, 0), (4, 3), (5, 1), (6, 2)):
                await_bytes(w_slot(m, dy, 1), w_r.at[m, k])

    def send_along_x(p):
        for dx in (2, 1, 3):
            send(
                rsx_s.at[dx, p], rsx_r.at[(-dx) % XN - 1, p],
                rx_s.at[dx - 1, p], rx_r.at[(-dx) % XN - 1, p], zx(0, dx), t,
            )

    def mixer(group):
        blocks = [(dx, ZPOS[dz]) for dx in range(XN) for dz in group]
        count = SUB * len(blocks)
        for dz in group:
            p = ZPOS[dz]
            if dz in NEXT:
                await_bytes(xbuf.at[:, p], gz_r.at[p - 1])
            elif dz in DIRECT_IN:
                if dz != 0:
                    for dx in range(XN):
                        await_bytes(xbuf.at[dx, p], az_r.at[dx, p])
            else:
                for dx in range(1, XN):
                    await_bytes(xbuf.at[dx, p], xf_r.at[dx - 1, p])
        for i, (dx, p) in enumerate(blocks):
            block = xbuf[dx, p].astype(F32)
            for j in range(TN):
                xs[SUB * i : SUB * (i + 1), DB * j : DB * (j + 1)] = block[j]
        sec = xs[:count, :]
        scale_two = lax.rsqrt(jnp.sum(sec * sec, axis=-1, keepdims=True) * (1.0 / D) + EPS)
        scaled = (sec * gains[...]).astype(BF16)
        preact = jnp.dot(scaled, upb[...], preferred_element_type=F32)
        hidden = jnp.square(jnp.maximum(preact * scale_two, 0.0)).astype(BF16)
        for j in range(TN):
            os[:count, DB * j : DB * (j + 1)] = jnp.dot(hidden, dnb[j], preferred_element_type=F32)
        for i, (dx, p) in enumerate(blocks):
            for j in range(TN):
                block = os[SUB * i : SUB * (i + 1), DB * j : DB * (j + 1)]
                if p == HOME:
                    own_row[dx, j] = block
                elif dx == 0 and ZORD[p] not in DIRECT_OUT + NEXT:
                    own[p, j] = block
                else:
                    rsx_s[dx, p, j] = block.astype(BF16)
        for dz in group:
            p = ZPOS[dz]
            if dz in DIRECT_OUT:
                for dx in (2, 1, 3, 0):
                    scatter(dz, dx, rsx_s.at[dx, p], fin, fi_s, fi_r)
            elif dz in NEXT:
                there = ZPOS[(-dz) % ZN] - 1
                send(rsx_s.at[:, p], rows_z.at[there], hz_s.at[p - 1], hz_r.at[there], zx(dz, 0), t)
            elif dz != 0:
                send_along_x(p)

    def sum_z():
        for k in range(2):
            await_bytes(rows_z.at[k], hz_r.at[k])
        for dx in range(XN):
            total = own_row[dx] + rows_z[0, dx].astype(F32) + rows_z[1, dx].astype(F32)
            if dx == 0:
                own[HOME] = total
            else:
                rsx_s[dx, HOME] = total.astype(BF16)
        send_along_x(HOME)

    def sum_x(p):
        for dx in range(1, XN):
            await_bytes(rsx_r.at[dx - 1, p], rx_r.at[dx - 1, p])
        total = own[p]
        for dx in range(1, XN):
            total += rsx_r[dx - 1, p].astype(F32)
        zs[p] = total.astype(BF16)
        scatter(ZORD[p], 0, zs.at[p], fin, fi_s, fi_r)

    for step in ORDER:
        group = [int(digit) for digit in step[1:]]
        if step == "w":
            rest_of_weights()
        elif step == "d":
            spread_row()
        elif step == "z":
            sum_z()
        elif step[0] == "r":
            relay(group[0], 2, 2, None)
        elif step[0] == "f":
            forward(group[0])
        elif step[0] == "m":
            mixer(group)
        else:
            sum_x(ZPOS[group[0]])

    for src, sem in pending:
        await_bytes(src, sem)
    for p in range(ZN):
        for dx in targets(ZORD[p], DIRECT_IN):
            count = TN - 1 if ZORD[p] == 0 and dx == 0 else TN
            await_bytes(seg.at[pl.ds(0, count)], az_s.at[dx, p])

    total = jnp.zeros((TN, SUB, DB), F32)
    for p in range(ZN):
        for dx in targets(ZORD[p], DIRECT_OUT):
            await_bytes(fin.at[dx, p], fi_r.at[dx, p])
            total += fin[dx, p].astype(F32)
    for s in range(TN):
        of[SUB * s : SUB * (s + 1), :] = total[s]
    out_ref[...] = (secf[...] + of[...]).astype(BF16)

    for p in range(ZN):
        for dx in targets(ZORD[p], DIRECT_OUT):
            count = TN - 1 if ZORD[p] == 0 and dx == 0 else TN
            await_bytes(seg.at[pl.ds(0, count)], fi_s.at[dx, p])
    store_mem.wait()


def write_out(*refs):
    ins, outs, sems = refs[:4], refs[4:8], refs[8]
    copies = [pltpu.make_async_copy(ins[k], outs[k], sems.at[k]) for k in (1, 0, 2, 3)]
    for copy in copies:
        copy.start()
    for copy in copies:
        copy.wait()


def per_device(
    tokens, memory, normalizer, stabilizer, norm_gain, query_weight, key_weight, value_weight, outgate_weight,
    input_gate_weight, forget_gate_weight, forget_bias, memory_gain, proj_weight, ffn_gain, up_weight, down_weight,
):
    hbm = pl.BlockSpec(memory_space=pltpu.HBM)
    anywhere = pl.BlockSpec(memory_space=pl.ANY)
    vmem = pl.BlockSpec(memory_space=pltpu.VMEM)
    dma = pltpu.SemaphoreType.DMA
    outs = (
        jax.ShapeDtypeStruct((ROWS, DB), BF16),
        jax.ShapeDtypeStruct((ROWS, DK, DK), F32),
        jax.ShapeDtypeStruct((ROWS, DK), F32),
        jax.ShapeDtypeStruct((1, ROWS), F32),
    )
    layer_out, memory_new, normalizer_new, stab_new = pl.pallas_call(
        kernel,
        out_shape=outs,
        in_specs=[hbm] * 17,
        out_specs=(vmem, anywhere, vmem, vmem),
        scratch_shapes=[
            pltpu.VMEM((ROWS, D), BF16),
            pltpu.VMEM((ROWS, DK, DK), F32),
            pltpu.VMEM((ROWS, DK), F32),
            pltpu.VMEM((1, ROWS), F32),
            pltpu.VMEM((1, D), F32),
            pltpu.VMEM((D, 4 * DK), BF16),
            pltpu.VMEM((TN, D), BF16),
            pltpu.VMEM((TN, D), BF16),
            pltpu.VMEM((1, TN), F32),
            pltpu.VMEM((1, DK), F32),
            pltpu.VMEM((TN * DK, DB), BF16),
            pltpu.VMEM((1, D), F32),
            pltpu.VMEM((D, FB), BF16),
            pltpu.VMEM((TN, FB, DB), BF16),
            pltpu.VMEM((ROWS, DK), F32),
            pltpu.VMEM((2, ROWS, DK), F32),
            pltpu.VMEM((DK, DK), F32),
            pltpu.VMEM((ROWS, TN * DK), BF16),
            pltpu.VMEM((ROWS, DB), F32),
            pltpu.VMEM((TN, SUB, DB), BF16),
            pltpu.VMEM((XN, ZN, TN, SUB, DB), BF16),
            pltpu.VMEM((ROWS, D), F32),
            pltpu.VMEM((ROWS, D), F32),
            pltpu.VMEM((XN, ZN, TN, SUB, DB), BF16),
            pltpu.VMEM((XN - 1, ZN, TN, SUB, DB), BF16),
            pltpu.VMEM((ZN, TN, SUB, DB), F32),
            pltpu.VMEM((XN, TN, SUB, DB), F32),
            pltpu.VMEM((2, XN, TN, SUB, DB), BF16),
            pltpu.VMEM((ZN, TN, SUB, DB), BF16),
            pltpu.VMEM((XN, ZN, TN, SUB, DB), BF16),
            pltpu.VMEM((ROWS, DB), F32),
            dma((18,)),
            dma((7,)), dma((7,)),
            dma((7,)), dma((7,)),
            dma((7,)), dma((7,)),
            dma((4, 7)), dma((4, 7)),
            dma((XN, ZN)), dma((XN, ZN)),
            dma((XN - 1, ZN)), dma((XN - 1, ZN)),
            dma((XN - 1, ZN)), dma((XN - 1, ZN)),
            dma((XN, ZN)), dma((XN, ZN)),
            dma((2,)), dma((2,)),
            dma((2,)), dma((2,)),
            pltpu.SemaphoreType.REGULAR((3,)),
            pltpu.SemaphoreType.REGULAR((2,)),
        ],
        compiler_params=pltpu.CompilerParams(
            collective_id=0, has_side_effects=True, vmem_limit_bytes=40 * 1024 * 1024
        ),
        name="layer",
    )(
        *(
            pltpu.with_memory_space_constraint(a, pltpu.HBM)
            for a in (
                tokens,
                memory.reshape(ROWS, DK, DK),
                normalizer.reshape(ROWS, DK),
                stabilizer.T,
                norm_gain.reshape(1, D),
                query_weight, key_weight, value_weight, outgate_weight,
                input_gate_weight.T,
                forget_gate_weight.T,
                forget_bias.reshape(1, TN),
                memory_gain.reshape(1, DK),
                proj_weight,
                ffn_gain.reshape(1, DB),
                up_weight,
                down_weight,
            )
        )
    )
    layer_out, memory_new, normalizer_new, stab_new = pl.pallas_call(
        write_out,
        out_shape=outs,
        in_specs=[anywhere] * 4,
        out_specs=(hbm,) * 4,
        scratch_shapes=[dma((4,))],
        compiler_params=pltpu.CompilerParams(vmem_limit_bytes=4 * 1024 * 1024),
        name="write_out",
    )(layer_out, memory_new, normalizer_new, stab_new)
    return (
        layer_out,
        memory_new.reshape(ROWS, 1, DK, DK),
        normalizer_new.reshape(ROWS, 1, DK),
        stab_new.T,
    )


def solution(mesh):
    placed = (
        P("kv", "tp"),
        P("kv", "tp", None, None),
        P("kv", "tp", None),
        P("kv", "tp"),
        P(),
        P(None, "tp"),
        P(None, "tp"),
        P(None, "tp"),
        P(None, "tp"),
        P(),
        P(),
        P(),
        P("tp"),
        P(None, "tp"),
        P("tp"),
        P("tp", "kv"),
        P("kv", "tp"),
    )
    outs = (P("kv", "tp"), P("kv", "tp", None, None), P("kv", "tp", None), P("kv", "tp"))
    return jax.shard_map(per_device, mesh=mesh, in_specs=placed, out_specs=outs, check_vma=False)
```

```python
import jax
import jax.numpy as jnp
from jax import lax
from jax.experimental import pallas as pl
from jax.experimental.pallas import tpu as pltpu
from jax.sharding import PartitionSpec as P

D = 2048
DK = 128
EPS = 1e-06
XN = 4
ZN = 8
YN = 4
TN = 8
ROWS = 32
DB = D // TN
SUB = ROWS // TN
FB = 256
ZORD = (0, 1, 7, 2, 6, 3, 5, 4)
ZSEND = (2, 6, 3, 5, 0, 4)
NEXT = (1, 7)
DIRECT_IN = (0,)
DIRECT_OUT = (4,)
ORDER = (
    "d", "f2", "f6", "r0", "r1", "f3", "f5", "r2", "r3", "f4", "w", "m17", "m26", "m35", "m4", "m0", "z", "s2", "s6", "s3", "s5", "s0",
)
ZPOS = tuple(ZORD.index(o) for o in range(ZN))
HOME = ZPOS[0]
TPO = ((2, 0), (2, 1), (1, 0), (1, 1), (3, 0), (3, 1), (0, 1))
F32 = jnp.float32
BF16 = jnp.bfloat16
MESH = pl.DeviceIdType.MESH


def remote(src, dst, send_sem, recv_sem, kv, tp):
    return pltpu.make_async_remote_copy(
        src_ref=src,
        dst_ref=dst,
        send_sem=send_sem,
        recv_sem=recv_sem,
        device_id={"kv": kv, "tp": tp},
        device_id_type=MESH,
    )


def await_bytes(ref, sem):
    pltpu.make_async_copy(ref, ref, sem).wait()


def kernel(
    tok_h, mem_h, nrm_h, stab_h, ng_h, qw_h, kw_h, vw_h, ow_h, ig_h, fg_h, fb_h, mg_h, pw_h, gain_h, up_h, dn_h,
    out_ref, memn_h, nrmn_ref, stabn_ref,
    tk, mem, nrm, stab, ng, qkvo, ig, fg, fb, mg, pw, gains, upb, dnb,
    qf, colrow, colmat, mx, secf, seg, xbuf, xs, os, rsx_s, rsx_r, own, own_row, rows_z, zs, fin, of,
    lsem, tok_s, tok_r, gain_s, gain_r, mix_s, mix_r, w_s, w_r, az_s, az_r, xf_s, xf_r, rx_s, rx_r, fi_s, fi_r, gz_s, gz_r, hz_s, hz_r,
    zready, xready,
):
    kv = lax.axis_index("kv")
    t = lax.axis_index("tp")
    z, x = kv // XN, kv % XN
    y, c = t // 2, t % 2

    def zx(dz, dx):
        return ((z + dz) % ZN) * XN + (x + dx) % XN

    def tp_at(dy, dc):
        return ((y + dy) % YN) * 2 + (c + dc) % 2

    pending = []

    def send(src, dst, ssem, rsem, kv_to, tp_to):
        remote(src, dst, ssem, rsem, kv_to, tp_to).start()
        pending.append((src, ssem))

    lane_t = pl.ds(pl.multiple_of(t * DB, DB), DB)
    lane_h = pl.ds(pl.multiple_of(t * DK, DK), DK)
    row_t = lane_t

    loads = {}

    def load(name, src, dst):
        k = len(loads)
        loads[name] = pltpu.make_async_copy(src, dst, lsem.at[k])
        loads[name].start()

    load("tok", tok_h, tk.at[:, lane_t])
    load("gain", gain_h, gains.at[:, lane_t])
    load("up", up_h, upb.at[row_t])
    load("dn", dn_h, dnb.at[t])
    load("ng", ng_h, ng)
    for k, (name, w) in enumerate((("q", qw_h), ("k", kw_h), ("v", vw_h), ("o", ow_h))):
        load(name, w, qkvo.at[:, DK * k : DK * (k + 1)])
    load("ig", ig_h, ig)
    load("fg", fg_h, fg)
    load("fb", fb_h, fb)
    load("stab", stab_h, stab)
    load("nrm", nrm_h, nrm)
    load("mem", mem_h, mem)
    load("mg", mg_h, mg)
    load("pw", pw_h, pw)

    def tell(sem, kv_to, tp_to):
        pl.semaphore_signal(sem, inc=1, device_id={"kv": kv_to, "tp": tp_to}, device_id_type=MESH)

    barrier = pltpu.get_barrier_semaphore()
    for dy, dc in TPO:
        tell(barrier, kv, tp_at(dy, dc))
    for step in (1, -1):
        tell(barrier, zx(0, step), t)
        tell(barrier, zx(step, 0), t)
    pl.semaphore_wait(barrier, 7 + 4)
    for step in (1, -1):
        tell(xready.at[0], zx(0, step), t)
        tell(zready.at[0], zx(step, 0), t)

    loads["tok"].wait()
    for k, (dy, dc) in enumerate(TPO):
        send(tk.at[:, lane_t], tk.at[:, lane_t], tok_s.at[k], tok_r.at[k], kv, tp_at(dy, dc))
    loads["gain"].wait()
    for k, (dy, dc) in enumerate(TPO):
        send(gains.at[:, lane_t], gains.at[:, lane_t], gain_s.at[k], gain_r.at[k], kv, tp_at(dy, dc))

    def w_slot(m, dy, dc):
        s = tp_at(dy, dc)
        if m < 2:
            return upb.at[pl.ds(pl.multiple_of(s * DB + DB // 2 * m, DB // 2), DB // 2)]
        return dnb.at[s, pl.ds(FB // 2 * (m - 2), FB // 2)]

    def send_weights(m):
        slot = w_slot(m, 0, 0)
        for k, (dy, dc) in ((0, (1, 0)), (1, (3, 0)), (3, (0, 1))):
            send(slot, slot, w_s.at[m, k], w_r.at[m, k], kv, tp_at(dy, dc))

    loads["up"].wait()
    send_weights(0)
    send_weights(1)

    pl.semaphore_wait(xready.at[0], 2)
    pl.semaphore_wait(zready.at[0], 2)
    for step in (2, -2):
        tell(zready.at[1], zx(step, 0), t)

    def chip_slice(dy, width):
        return pl.ds(pl.multiple_of(((y - dy) % YN) * 2 * width, 2 * width), 2 * width)

    def await_chip(dy, recv):
        for k, (other, dc) in enumerate(TPO):
            if other == dy:
                await_bytes(recv[0](tp_at(-dy, -dc)), recv[1].at[k])

    for name in ("ng", "q", "k", "v", "o", "ig", "fg", "fb", "stab", "nrm"):
        loads[name].wait()
    contract = (((1,), (1,)), ((), ()))
    square_sum = jnp.zeros((ROWS, 1), F32)
    proj4 = jnp.zeros((ROWS, 4 * DK), F32)
    all_in = jnp.zeros((ROWS, TN), F32)
    all_forget = jnp.zeros((ROWS, TN), F32)
    for dy in (0, 1, 3, 2):
        if dy == 1:
            pl.semaphore_wait(zready.at[1], 2)
            for step in (3, -3, 4):
                tell(zready.at[2], zx(step, 0), t)
        await_chip(dy, (lambda s: tk.at[:, pl.ds(pl.multiple_of(s * DB, DB), DB)], tok_r))
        cols = chip_slice(dy, DB)
        rows = tk[:, cols].astype(F32)
        square_sum += jnp.sum(rows * rows, axis=-1, keepdims=True)
        gained = (rows * ng[:, cols]).astype(BF16)
        proj4 += jnp.dot(gained, qkvo[cols, :], preferred_element_type=F32)
        all_in += lax.dot_general(gained, ig[:, cols], contract, preferred_element_type=F32)
        all_forget += lax.dot_general(gained, fg[:, cols], contract, preferred_element_type=F32)
    scale_one = lax.rsqrt(square_sum * (1.0 / D) + EPS)
    proj4 = (proj4 * scale_one).astype(BF16).astype(F32)
    query = proj4[:, :DK]
    keys = proj4[:, DK : 2 * DK] * DK ** (-0.5)
    values = proj4[:, 2 * DK : 3 * DK]
    gate_out = proj4[:, 3 * DK :]
    qf[...] = query

    all_in = all_in * scale_one
    all_forget = all_forget * scale_one + fb[...]
    head = lax.broadcasted_iota(jnp.int32, (ROWS, TN), 1) == t
    input_log = jnp.sum(jnp.where(head, all_in, 0.0), axis=1, keepdims=True)
    raw = jnp.sum(jnp.where(head, all_forget, 0.0), axis=1, keepdims=True)
    forget_log = jnp.minimum(raw, 0.0) - jnp.log1p(jnp.exp(-jnp.abs(raw)))
    diag = lax.broadcasted_iota(jnp.int32, (ROWS, ROWS), 0) == lax.broadcasted_iota(jnp.int32, (ROWS, ROWS), 1)
    stab_col = jnp.sum(jnp.where(diag, jnp.broadcast_to(stab[...], (ROWS, ROWS)), 0.0), axis=1, keepdims=True)
    stab_new = jnp.maximum(forget_log + stab_col, input_log)
    keep = jnp.exp(forget_log + stab_col - stab_new)
    admit = jnp.exp(input_log - stab_new)
    normalizer_new = keep * nrm[...] + admit * keys
    denom = jnp.sum(normalizer_new * query, axis=1, keepdims=True)
    key_query = jnp.sum(keys * query, axis=1, keepdims=True)

    loads["mem"].wait()
    lane = lax.broadcasted_iota(jnp.int32, (DK, DK), 1)

    def read_memory(b, acc):
        part = jnp.sum(mem[b] * qf[pl.ds(b, 1), :], axis=1, keepdims=True)
        return jnp.where(lane == b, part, acc)

    ones = jnp.ones((DK, DK), BF16)
    read = jnp.zeros((DK, DK), F32)
    for first in range(0, ROWS // 2, 4):
        product = jnp.concatenate([mem[b] * qf[b : b + 1, :] for b in range(first, first + 4)], axis=0)
        high = product.astype(BF16)
        low = (product - high.astype(F32)).astype(BF16)
        sums = jnp.dot(high, ones, preferred_element_type=F32) + jnp.dot(low, ones, preferred_element_type=F32)
        for k in range(4):
            read = jnp.where(lane == first + k, sums[DK * k : DK * (k + 1), :], read)
        for b in range(ROWS // 2 + first, ROWS // 2 + first + 4):
            read = read_memory(b, read)
    memory_query = read.T[:ROWS, :]
    numer = keep * memory_query + (admit * key_query) * values
    cell = numer / jnp.maximum(jnp.abs(denom), 1.0)
    loads["mg"].wait()
    mx[:, lane_h] = (cell * mg[...] * jax.nn.sigmoid(gate_out)).astype(BF16)
    for k, (dy, dc) in enumerate(TPO):
        send(mx.at[:, lane_h], mx.at[:, lane_h], mix_s.at[k], mix_r.at[k], kv, tp_at(dy, dc))

    loads["dn"].wait()
    send_weights(2)
    send_weights(3)
    nrmn_ref[...] = normalizer_new
    stabn_ref[...] = jnp.sum(
        jnp.where(diag, jnp.broadcast_to(stab_new, (ROWS, ROWS)), 0.0), axis=0, keepdims=True
    )
    colrow[0] = jnp.broadcast_to(keep, (ROWS, DK))
    colrow[1] = keys
    colmat[:ROWS, :] = admit * values
    colmat[ROWS:, :] = jnp.zeros((DK - ROWS, DK), F32)
    admitted = colmat[...].T

    def write_memory(b, carry):
        column = jnp.sum(jnp.where(lane == b, admitted, 0.0), axis=1, keepdims=True)
        mem[b] = colrow[0, pl.ds(b, 1), :] * mem[b] + column * colrow[1, pl.ds(b, 1), :]
        return carry

    lax.fori_loop(0, ROWS, write_memory, 0, unroll=ROWS)
    store_mem = pltpu.make_async_copy(mem, memn_h, lsem.at[len(loads)])
    store_mem.start()

    pl.semaphore_wait(zready.at[2], 3)
    for dx in range(1, XN):
        tell(xready.at[1], zx(0, dx), t)

    def relay(m, k, dy, forward):
        slot = w_slot(m, dy, 0)
        await_bytes(slot, w_r.at[m, k])
        if forward is not None:
            send(slot, slot, w_s.at[m, 2], w_r.at[m, 2], kv, tp_at(forward, 0))
        send(slot, slot, w_s.at[m, 4 + k], w_r.at[m, 4 + k], kv, tp_at(0, 1))

    loads["pw"].wait()
    projected = jnp.zeros((ROWS, DB), F32)
    for dy in (0, 1, 3, 2):
        await_chip(dy, (lambda s: mx.at[:, pl.ds(pl.multiple_of(s * DK, DK), DK)], mix_r))
        cols = chip_slice(dy, DK)
        projected += jnp.dot(mx[:, cols], pw[cols, :], preferred_element_type=F32)
    second = (tk[:, lane_t].astype(F32) + projected).astype(BF16).astype(F32)
    secf[...] = second
    for s in range(TN):
        seg[s] = secf[SUB * s : SUB * (s + 1), :].astype(BF16)

    def scatter(dz, dx, src, dst, ssem, rsem):
        there = ZPOS[(-dz) % ZN]
        slot = (-dx) % XN
        for dy, dc in TPO + ((0, 0),):
            s = tp_at(dy, dc)
            if dz == 0 and dx == 0 and (dy, dc) == (0, 0):
                pltpu.make_async_copy(src.at[s], dst.at[slot, there, t], rsem.at[slot, there]).start()
            else:
                remote(
                    src.at[s], dst.at[slot, there, t], ssem.at[dx, ZPOS[dz]], rsem.at[slot, there], zx(dz, dx), s
                ).start()

    def targets(dz, direct):
        if dz in NEXT:
            return ()
        return (2, 1, 3, 0) if dz in direct else (0,)

    pl.semaphore_wait(xready.at[1], XN - 1)
    for dz in ZSEND:
        for dx in targets(dz, DIRECT_IN):
            scatter(dz, dx, seg, xbuf, az_s, az_r)

    relay(0, 0, 3, 1)
    relay(1, 1, 1, 3)
    relay(0, 1, 1, None)
    relay(1, 0, 3, None)
    relay(2, 1, 1, 3)
    relay(3, 0, 3, 1)
    relay(2, 0, 3, None)
    relay(3, 1, 1, None)

    def forward(dz):
        p = ZPOS[dz]
        await_bytes(xbuf.at[0, p], az_r.at[0, p])
        for dx in (2, 1, 3):
            send(
                xbuf.at[0, p], xbuf.at[(-dx) % XN, p],
                xf_s.at[dx - 1, p], xf_r.at[(-dx) % XN - 1, p], zx(0, dx), t,
            )

    def spread_row():
        for dx in range(XN):
            await_bytes(xbuf.at[dx, HOME], az_r.at[dx, HOME])
        for k, dz in enumerate(NEXT):
            there = ZPOS[(-dz) % ZN]
            send(xbuf.at[:, HOME], xbuf.at[:, there], gz_s.at[k], gz_r.at[there - 1], zx(dz, 0), t)

    def rest_of_weights():
        for k, (dy, dc) in enumerate(TPO):
            s = tp_at(-dy, -dc)
            await_bytes(gains.at[:, pl.ds(pl.multiple_of(s * DB, DB), DB)], gain_r.at[k])
        for m in range(4):
            for k, dy in ((3, 0), (4, 3), (5, 1), (6, 2)):
                await_bytes(w_slot(m, dy, 1), w_r.at[m, k])

    def send_along_x(p):
        for dx in (2, 1, 3):
            send(
                rsx_s.at[dx, p], rsx_r.at[(-dx) % XN - 1, p],
                rx_s.at[dx - 1, p], rx_r.at[(-dx) % XN - 1, p], zx(0, dx), t,
            )

    def mixer(group):
        blocks = [(dx, ZPOS[dz]) for dx in range(XN) for dz in group]
        count = SUB * len(blocks)
        for dz in group:
            p = ZPOS[dz]
            if dz in NEXT:
                await_bytes(xbuf.at[:, p], gz_r.at[p - 1])
            elif dz in DIRECT_IN:
                if dz != 0:
                    for dx in range(XN):
                        await_bytes(xbuf.at[dx, p], az_r.at[dx, p])
            else:
                for dx in range(1, XN):
                    await_bytes(xbuf.at[dx, p], xf_r.at[dx - 1, p])
        for i, (dx, p) in enumerate(blocks):
            block = xbuf[dx, p].astype(F32)
            for j in range(TN):
                xs[SUB * i : SUB * (i + 1), DB * j : DB * (j + 1)] = block[j]
        sec = xs[:count, :]
        scale_two = lax.rsqrt(jnp.sum(sec * sec, axis=-1, keepdims=True) * (1.0 / D) + EPS)
        scaled = (sec * gains[...]).astype(BF16)
        preact = jnp.dot(scaled, upb[...], preferred_element_type=F32)
        hidden = jnp.square(jnp.maximum(preact * scale_two, 0.0)).astype(BF16)
        for j in range(TN):
            os[:count, DB * j : DB * (j + 1)] = jnp.dot(hidden, dnb[j], preferred_element_type=F32)
        for i, (dx, p) in enumerate(blocks):
            for j in range(TN):
                block = os[SUB * i : SUB * (i + 1), DB * j : DB * (j + 1)]
                if p == HOME:
                    own_row[dx, j] = block
                elif dx == 0 and ZORD[p] not in DIRECT_OUT + NEXT:
                    own[p, j] = block
                else:
                    rsx_s[dx, p, j] = block.astype(BF16)
        for dz in group:
            p = ZPOS[dz]
            if dz in DIRECT_OUT:
                for dx in (2, 1, 3, 0):
                    scatter(dz, dx, rsx_s.at[dx, p], fin, fi_s, fi_r)
            elif dz in NEXT:
                there = ZPOS[(-dz) % ZN] - 1
                send(rsx_s.at[:, p], rows_z.at[there], hz_s.at[p - 1], hz_r.at[there], zx(dz, 0), t)
            elif dz != 0:
                send_along_x(p)

    def sum_z():
        for k in range(2):
            await_bytes(rows_z.at[k], hz_r.at[k])
        for dx in range(XN):
            total = own_row[dx] + rows_z[0, dx].astype(F32) + rows_z[1, dx].astype(F32)
            if dx == 0:
                own[HOME] = total
            else:
                rsx_s[dx, HOME] = total.astype(BF16)
        send_along_x(HOME)

    def sum_x(p):
        for dx in range(1, XN):
            await_bytes(rsx_r.at[dx - 1, p], rx_r.at[dx - 1, p])
        total = own[p]
        for dx in range(1, XN):
            total += rsx_r[dx - 1, p].astype(F32)
        zs[p] = total.astype(BF16)
        scatter(ZORD[p], 0, zs.at[p], fin, fi_s, fi_r)

    for step in ORDER:
        group = [int(digit) for digit in step[1:]]
        if step == "w":
            rest_of_weights()
        elif step == "d":
            spread_row()
        elif step == "z":
            sum_z()
        elif step[0] == "r":
            relay(group[0], 2, 2, None)
        elif step[0] == "f":
            forward(group[0])
        elif step[0] == "m":
            mixer(group)
        else:
            sum_x(ZPOS[group[0]])

    for src, sem in pending:
        await_bytes(src, sem)
    for p in range(ZN):
        for dx in targets(ZORD[p], DIRECT_IN):
            count = TN - 1 if ZORD[p] == 0 and dx == 0 else TN
            await_bytes(seg.at[pl.ds(0, count)], az_s.at[dx, p])

    total = jnp.zeros((TN, SUB, DB), F32)
    for p in range(ZN):
        for dx in targets(ZORD[p], DIRECT_OUT):
            await_bytes(fin.at[dx, p], fi_r.at[dx, p])
            total += fin[dx, p].astype(F32)
    for s in range(TN):
        of[SUB * s : SUB * (s + 1), :] = total[s]
    out_ref[...] = (secf[...] + of[...]).astype(BF16)

    for p in range(ZN):
        for dx in targets(ZORD[p], DIRECT_OUT):
            count = TN - 1 if ZORD[p] == 0 and dx == 0 else TN
            await_bytes(seg.at[pl.ds(0, count)], fi_s.at[dx, p])
    store_mem.wait()


def write_out(*refs):
    ins, outs, sems = refs[:4], refs[4:8], refs[8]
    copies = [pltpu.make_async_copy(ins[k], outs[k], sems.at[k]) for k in (1, 0, 2, 3)]
    for copy in copies:
        copy.start()
    for copy in copies:
        copy.wait()


def per_device(
    tokens, memory, normalizer, stabilizer, norm_gain, query_weight, key_weight, value_weight, outgate_weight,
    input_gate_weight, forget_gate_weight, forget_bias, memory_gain, proj_weight, ffn_gain, up_weight, down_weight,
):
    hbm = pl.BlockSpec(memory_space=pltpu.HBM)
    anywhere = pl.BlockSpec(memory_space=pl.ANY)
    vmem = pl.BlockSpec(memory_space=pltpu.VMEM)
    dma = pltpu.SemaphoreType.DMA
    outs = (
        jax.ShapeDtypeStruct((ROWS, DB), BF16),
        jax.ShapeDtypeStruct((ROWS, DK, DK), F32),
        jax.ShapeDtypeStruct((ROWS, DK), F32),
        jax.ShapeDtypeStruct((1, ROWS), F32),
    )
    layer_out, memory_new, normalizer_new, stab_new = pl.pallas_call(
        kernel,
        out_shape=outs,
        in_specs=[hbm] * 17,
        out_specs=(vmem, anywhere, vmem, vmem),
        scratch_shapes=[
            pltpu.VMEM((ROWS, D), BF16),
            pltpu.VMEM((ROWS, DK, DK), F32),
            pltpu.VMEM((ROWS, DK), F32),
            pltpu.VMEM((1, ROWS), F32),
            pltpu.VMEM((1, D), F32),
            pltpu.VMEM((D, 4 * DK), BF16),
            pltpu.VMEM((TN, D), BF16),
            pltpu.VMEM((TN, D), BF16),
            pltpu.VMEM((1, TN), F32),
            pltpu.VMEM((1, DK), F32),
            pltpu.VMEM((TN * DK, DB), BF16),
            pltpu.VMEM((1, D), F32),
            pltpu.VMEM((D, FB), BF16),
            pltpu.VMEM((TN, FB, DB), BF16),
            pltpu.VMEM((ROWS, DK), F32),
            pltpu.VMEM((2, ROWS, DK), F32),
            pltpu.VMEM((DK, DK), F32),
            pltpu.VMEM((ROWS, TN * DK), BF16),
            pltpu.VMEM((ROWS, DB), F32),
            pltpu.VMEM((TN, SUB, DB), BF16),
            pltpu.VMEM((XN, ZN, TN, SUB, DB), BF16),
            pltpu.VMEM((ROWS, D), F32),
            pltpu.VMEM((ROWS, D), F32),
            pltpu.VMEM((XN, ZN, TN, SUB, DB), BF16),
            pltpu.VMEM((XN - 1, ZN, TN, SUB, DB), BF16),
            pltpu.VMEM((ZN, TN, SUB, DB), F32),
            pltpu.VMEM((XN, TN, SUB, DB), F32),
            pltpu.VMEM((2, XN, TN, SUB, DB), BF16),
            pltpu.VMEM((ZN, TN, SUB, DB), BF16),
            pltpu.VMEM((XN, ZN, TN, SUB, DB), BF16),
            pltpu.VMEM((ROWS, DB), F32),
            dma((18,)),
            dma((7,)), dma((7,)),
            dma((7,)), dma((7,)),
            dma((7,)), dma((7,)),
            dma((4, 7)), dma((4, 7)),
            dma((XN, ZN)), dma((XN, ZN)),
            dma((XN - 1, ZN)), dma((XN - 1, ZN)),
            dma((XN - 1, ZN)), dma((XN - 1, ZN)),
            dma((XN, ZN)), dma((XN, ZN)),
            dma((2,)), dma((2,)),
            dma((2,)), dma((2,)),
            pltpu.SemaphoreType.REGULAR((3,)),
            pltpu.SemaphoreType.REGULAR((2,)),
        ],
        compiler_params=pltpu.CompilerParams(
            collective_id=0, has_side_effects=True, vmem_limit_bytes=40 * 1024 * 1024
        ),
        name="layer",
    )(
        *(
            pltpu.with_memory_space_constraint(a, pltpu.HBM)
            for a in (
                tokens,
                memory.reshape(ROWS, DK, DK),
                normalizer.reshape(ROWS, DK),
                stabilizer.T,
                norm_gain.reshape(1, D),
                query_weight, key_weight, value_weight, outgate_weight,
                input_gate_weight.T,
                forget_gate_weight.T,
                forget_bias.reshape(1, TN),
                memory_gain.reshape(1, DK),
                proj_weight,
                ffn_gain.reshape(1, DB),
                up_weight,
                down_weight,
            )
        )
    )
    layer_out, memory_new, normalizer_new, stab_new = pl.pallas_call(
        write_out,
        out_shape=outs,
        in_specs=[anywhere] * 4,
        out_specs=(hbm,) * 4,
        scratch_shapes=[dma((4,))],
        compiler_params=pltpu.CompilerParams(vmem_limit_bytes=4 * 1024 * 1024),
        name="write_out",
    )(layer_out, memory_new, normalizer_new, stab_new)
    return (
        layer_out,
        memory_new.reshape(ROWS, 1, DK, DK),
        normalizer_new.reshape(ROWS, 1, DK),
        stab_new.T,
    )


def solution(mesh):
    placed = (
        P("kv", "tp"),
        P("kv", "tp", None, None),
        P("kv", "tp", None),
        P("kv", "tp"),
        P(),
        P(None, "tp"),
        P(None, "tp"),
        P(None, "tp"),
        P(None, "tp"),
        P(),
        P(),
        P(),
        P("tp"),
        P(None, "tp"),
        P("tp"),
        P("tp", "kv"),
        P("kv", "tp"),
    )
    outs = (P("kv", "tp"), P("kv", "tp", None, None), P("kv", "tp", None), P("kv", "tp"))
    return jax.shard_map(per_device, mesh=mesh, in_specs=placed, out_specs=outs, check_vma=False)
```

```python
import jax
import jax.numpy as jnp
from jax import lax
from jax.experimental import pallas as pl
from jax.experimental.pallas import tpu as pltpu
from jax.sharding import PartitionSpec as P

D = 2048
DK = 128
EPS = 1e-06
XN = 4
ZN = 8
YN = 4
TN = 8
ROWS = 32
DB = D // TN
SUB = ROWS // TN
FB = 256
ZORD = (0, 1, 7, 2, 6, 3, 5, 4)
ZSEND = (2, 6, 3, 5, 0, 4)
NEXT = (1, 7)
DIRECT_IN = (0,)
DIRECT_OUT = (4,)
ORDER = (
    "d", "f2", "f6", "f3", "f5", "r0", "r1", "r2", "r3", "f4", "w", "m17", "m26", "m35", "m4", "m0", "z", "s2", "s6", "s3", "s5", "s0",
)
ZPOS = tuple(ZORD.index(o) for o in range(ZN))
HOME = ZPOS[0]
TPO = ((2, 0), (2, 1), (1, 0), (1, 1), (3, 0), (3, 1), (0, 1))
F32 = jnp.float32
BF16 = jnp.bfloat16
MESH = pl.DeviceIdType.MESH


def remote(src, dst, send_sem, recv_sem, kv, tp):
    return pltpu.make_async_remote_copy(
        src_ref=src,
        dst_ref=dst,
        send_sem=send_sem,
        recv_sem=recv_sem,
        device_id={"kv": kv, "tp": tp},
        device_id_type=MESH,
    )


def await_bytes(ref, sem):
    pltpu.make_async_copy(ref, ref, sem).wait()


def kernel(
    tok_h, mem_h, nrm_h, stab_h, ng_h, qw_h, kw_h, vw_h, ow_h, ig_h, fg_h, fb_h, mg_h, pw_h, gain_h, up_h, dn_h,
    out_ref, memn_h, nrmn_ref, stabn_ref,
    tk, mem, nrm, stab, ng, qkvo, ig, fg, fb, mg, pw, gains, upb, dnb,
    qf, colrow, colmat, mx, secf, seg, xbuf, xs, os, rsx_s, rsx_r, own, own_row, rows_z, zs, fin, of,
    lsem, tok_s, tok_r, gain_s, gain_r, mix_s, mix_r, w_s, w_r, az_s, az_r, xf_s, xf_r, rx_s, rx_r, fi_s, fi_r, gz_s, gz_r, hz_s, hz_r,
    zready, xready,
):
    kv = lax.axis_index("kv")
    t = lax.axis_index("tp")
    z, x = kv // XN, kv % XN
    y, c = t // 2, t % 2

    def zx(dz, dx):
        return ((z + dz) % ZN) * XN + (x + dx) % XN

    def tp_at(dy, dc):
        return ((y + dy) % YN) * 2 + (c + dc) % 2

    pending = []

    def send(src, dst, ssem, rsem, kv_to, tp_to):
        remote(src, dst, ssem, rsem, kv_to, tp_to).start()
        pending.append((src, ssem))

    lane_t = pl.ds(pl.multiple_of(t * DB, DB), DB)
    lane_h = pl.ds(pl.multiple_of(t * DK, DK), DK)
    row_t = lane_t

    loads = {}

    def load(name, src, dst):
        k = len(loads)
        loads[name] = pltpu.make_async_copy(src, dst, lsem.at[k])
        loads[name].start()

    load("tok", tok_h, tk.at[:, lane_t])
    load("gain", gain_h, gains.at[:, lane_t])
    load("up", up_h, upb.at[row_t])
    load("dn", dn_h, dnb.at[t])
    load("ng", ng_h, ng)
    for k, (name, w) in enumerate((("q", qw_h), ("k", kw_h), ("v", vw_h), ("o", ow_h))):
        load(name, w, qkvo.at[:, DK * k : DK * (k + 1)])
    load("ig", ig_h, ig)
    load("fg", fg_h, fg)
    load("fb", fb_h, fb)
    load("stab", stab_h, stab)
    load("nrm", nrm_h, nrm)
    load("mem", mem_h, mem)
    load("mg", mg_h, mg)
    load("pw", pw_h, pw)

    def tell(sem, kv_to, tp_to):
        pl.semaphore_signal(sem, inc=1, device_id={"kv": kv_to, "tp": tp_to}, device_id_type=MESH)

    barrier = pltpu.get_barrier_semaphore()
    for dy, dc in TPO:
        tell(barrier, kv, tp_at(dy, dc))
    for step in (1, -1):
        tell(barrier, zx(0, step), t)
        tell(barrier, zx(step, 0), t)
    pl.semaphore_wait(barrier, 7 + 4)
    for step in (1, -1):
        tell(xready.at[0], zx(0, step), t)
        tell(zready.at[0], zx(step, 0), t)

    loads["tok"].wait()
    for k, (dy, dc) in enumerate(TPO):
        send(tk.at[:, lane_t], tk.at[:, lane_t], tok_s.at[k], tok_r.at[k], kv, tp_at(dy, dc))
    loads["gain"].wait()
    for k, (dy, dc) in enumerate(TPO):
        send(gains.at[:, lane_t], gains.at[:, lane_t], gain_s.at[k], gain_r.at[k], kv, tp_at(dy, dc))

    def w_slot(m, dy, dc):
        s = tp_at(dy, dc)
        if m < 2:
            return upb.at[pl.ds(pl.multiple_of(s * DB + DB // 2 * m, DB // 2), DB // 2)]
        return dnb.at[s, pl.ds(FB // 2 * (m - 2), FB // 2)]

    def send_weights(m):
        slot = w_slot(m, 0, 0)
        for k, (dy, dc) in ((0, (1, 0)), (1, (3, 0)), (3, (0, 1))):
            send(slot, slot, w_s.at[m, k], w_r.at[m, k], kv, tp_at(dy, dc))

    loads["up"].wait()
    send_weights(0)
    send_weights(1)

    pl.semaphore_wait(xready.at[0], 2)
    pl.semaphore_wait(zready.at[0], 2)
    for step in (2, -2):
        tell(zready.at[1], zx(step, 0), t)

    def chip_slice(dy, width):
        return pl.ds(pl.multiple_of(((y - dy) % YN) * 2 * width, 2 * width), 2 * width)

    def await_chip(dy, recv):
        for k, (other, dc) in enumerate(TPO):
            if other == dy:
                await_bytes(recv[0](tp_at(-dy, -dc)), recv[1].at[k])

    for name in ("ng", "q", "k", "v", "o", "ig", "fg", "fb", "stab", "nrm"):
        loads[name].wait()
    contract = (((1,), (1,)), ((), ()))
    square_sum = jnp.zeros((ROWS, 1), F32)
    proj4 = jnp.zeros((ROWS, 4 * DK), F32)
    all_in = jnp.zeros((ROWS, TN), F32)
    all_forget = jnp.zeros((ROWS, TN), F32)
    for dy in (0, 1, 3, 2):
        if dy == 1:
            pl.semaphore_wait(zready.at[1], 2)
            for step in (3, -3, 4):
                tell(zready.at[2], zx(step, 0), t)
        await_chip(dy, (lambda s: tk.at[:, pl.ds(pl.multiple_of(s * DB, DB), DB)], tok_r))
        cols = chip_slice(dy, DB)
        rows = tk[:, cols].astype(F32)
        square_sum += jnp.sum(rows * rows, axis=-1, keepdims=True)
        gained = (rows * ng[:, cols]).astype(BF16)
        proj4 += jnp.dot(gained, qkvo[cols, :], preferred_element_type=F32)
        all_in += lax.dot_general(gained, ig[:, cols], contract, preferred_element_type=F32)
        all_forget += lax.dot_general(gained, fg[:, cols], contract, preferred_element_type=F32)
    scale_one = lax.rsqrt(square_sum * (1.0 / D) + EPS)
    proj4 = (proj4 * scale_one).astype(BF16).astype(F32)
    query = proj4[:, :DK]
    keys = proj4[:, DK : 2 * DK] * DK ** (-0.5)
    values = proj4[:, 2 * DK : 3 * DK]
    gate_out = proj4[:, 3 * DK :]
    qf[...] = query

    all_in = all_in * scale_one
    all_forget = all_forget * scale_one + fb[...]
    head = lax.broadcasted_iota(jnp.int32, (ROWS, TN), 1) == t
    input_log = jnp.sum(jnp.where(head, all_in, 0.0), axis=1, keepdims=True)
    raw = jnp.sum(jnp.where(head, all_forget, 0.0), axis=1, keepdims=True)
    forget_log = jnp.minimum(raw, 0.0) - jnp.log1p(jnp.exp(-jnp.abs(raw)))
    diag = lax.broadcasted_iota(jnp.int32, (ROWS, ROWS), 0) == lax.broadcasted_iota(jnp.int32, (ROWS, ROWS), 1)
    stab_col = jnp.sum(jnp.where(diag, jnp.broadcast_to(stab[...], (ROWS, ROWS)), 0.0), axis=1, keepdims=True)
    stab_new = jnp.maximum(forget_log + stab_col, input_log)
    keep = jnp.exp(forget_log + stab_col - stab_new)
    admit = jnp.exp(input_log - stab_new)
    normalizer_new = keep * nrm[...] + admit * keys
    denom = jnp.sum(normalizer_new * query, axis=1, keepdims=True)
    key_query = jnp.sum(keys * query, axis=1, keepdims=True)

    loads["mem"].wait()
    lane = lax.broadcasted_iota(jnp.int32, (DK, DK), 1)

    def read_memory(b, acc):
        part = jnp.sum(mem[b] * qf[pl.ds(b, 1), :], axis=1, keepdims=True)
        return jnp.where(lane == b, part, acc)

    ones = jnp.ones((DK, DK), BF16)
    read = jnp.zeros((DK, DK), F32)
    for first in range(0, ROWS // 2, 4):
        product = jnp.concatenate([mem[b] * qf[b : b + 1, :] for b in range(first, first + 4)], axis=0)
        high = product.astype(BF16)
        low = (product - high.astype(F32)).astype(BF16)
        sums = jnp.dot(high, ones, preferred_element_type=F32) + jnp.dot(low, ones, preferred_element_type=F32)
        for k in range(4):
            read = jnp.where(lane == first + k, sums[DK * k : DK * (k + 1), :], read)
        for b in range(ROWS // 2 + first, ROWS // 2 + first + 4):
            read = read_memory(b, read)
    memory_query = read.T[:ROWS, :]
    numer = keep * memory_query + (admit * key_query) * values
    cell = numer / jnp.maximum(jnp.abs(denom), 1.0)
    loads["mg"].wait()
    mx[:, lane_h] = (cell * mg[...] * jax.nn.sigmoid(gate_out)).astype(BF16)
    for k, (dy, dc) in enumerate(TPO):
        send(mx.at[:, lane_h], mx.at[:, lane_h], mix_s.at[k], mix_r.at[k], kv, tp_at(dy, dc))

    loads["dn"].wait()
    send_weights(2)
    send_weights(3)
    nrmn_ref[...] = normalizer_new
    stabn_ref[...] = jnp.sum(
        jnp.where(diag, jnp.broadcast_to(stab_new, (ROWS, ROWS)), 0.0), axis=0, keepdims=True
    )
    colrow[0] = jnp.broadcast_to(keep, (ROWS, DK))
    colrow[1] = keys
    colmat[:ROWS, :] = admit * values
    colmat[ROWS:, :] = jnp.zeros((DK - ROWS, DK), F32)
    admitted = colmat[...].T

    def write_memory(b, carry):
        column = jnp.sum(jnp.where(lane == b, admitted, 0.0), axis=1, keepdims=True)
        mem[b] = colrow[0, pl.ds(b, 1), :] * mem[b] + column * colrow[1, pl.ds(b, 1), :]
        return carry

    lax.fori_loop(0, ROWS, write_memory, 0, unroll=ROWS)
    store_mem = pltpu.make_async_copy(mem, memn_h, lsem.at[len(loads)])
    store_mem.start()

    pl.semaphore_wait(zready.at[2], 3)
    for dx in range(1, XN):
        tell(xready.at[1], zx(0, dx), t)

    def relay(m, k, dy, forward):
        slot = w_slot(m, dy, 0)
        await_bytes(slot, w_r.at[m, k])
        if forward is not None:
            send(slot, slot, w_s.at[m, 2], w_r.at[m, 2], kv, tp_at(forward, 0))
        send(slot, slot, w_s.at[m, 4 + k], w_r.at[m, 4 + k], kv, tp_at(0, 1))

    loads["pw"].wait()
    projected = jnp.zeros((ROWS, DB), F32)
    for dy in (0, 1, 3, 2):
        await_chip(dy, (lambda s: mx.at[:, pl.ds(pl.multiple_of(s * DK, DK), DK)], mix_r))
        cols = chip_slice(dy, DK)
        projected += jnp.dot(mx[:, cols], pw[cols, :], preferred_element_type=F32)
    second = (tk[:, lane_t].astype(F32) + projected).astype(BF16).astype(F32)
    secf[...] = second
    for s in range(TN):
        seg[s] = secf[SUB * s : SUB * (s + 1), :].astype(BF16)

    def scatter(dz, dx, src, dst, ssem, rsem):
        there = ZPOS[(-dz) % ZN]
        slot = (-dx) % XN
        for dy, dc in TPO + ((0, 0),):
            s = tp_at(dy, dc)
            if dz == 0 and dx == 0 and (dy, dc) == (0, 0):
                pltpu.make_async_copy(src.at[s], dst.at[slot, there, t], rsem.at[slot, there]).start()
            else:
                remote(
                    src.at[s], dst.at[slot, there, t], ssem.at[dx, ZPOS[dz]], rsem.at[slot, there], zx(dz, dx), s
                ).start()

    def targets(dz, direct):
        if dz in NEXT:
            return ()
        return (2, 1, 3, 0) if dz in direct else (0,)

    pl.semaphore_wait(xready.at[1], XN - 1)
    for dz in ZSEND:
        for dx in targets(dz, DIRECT_IN):
            scatter(dz, dx, seg, xbuf, az_s, az_r)

    relay(0, 0, 3, 1)
    relay(1, 1, 1, 3)
    relay(0, 1, 1, None)
    relay(1, 0, 3, None)
    relay(2, 1, 1, 3)
    relay(3, 0, 3, 1)
    relay(2, 0, 3, None)
    relay(3, 1, 1, None)

    def forward(dz):
        p = ZPOS[dz]
        await_bytes(xbuf.at[0, p], az_r.at[0, p])
        for dx in (2, 1, 3):
            send(
                xbuf.at[0, p], xbuf.at[(-dx) % XN, p],
                xf_s.at[dx - 1, p], xf_r.at[(-dx) % XN - 1, p], zx(0, dx), t,
            )

    def spread_row():
        for dx in range(XN):
            await_bytes(xbuf.at[dx, HOME], az_r.at[dx, HOME])
        for k, dz in enumerate(NEXT):
            there = ZPOS[(-dz) % ZN]
            send(xbuf.at[:, HOME], xbuf.at[:, there], gz_s.at[k], gz_r.at[there - 1], zx(dz, 0), t)

    def rest_of_weights():
        for k, (dy, dc) in enumerate(TPO):
            s = tp_at(-dy, -dc)
            await_bytes(gains.at[:, pl.ds(pl.multiple_of(s * DB, DB), DB)], gain_r.at[k])
        for m in range(4):
            for k, dy in ((3, 0), (4, 3), (5, 1), (6, 2)):
                await_bytes(w_slot(m, dy, 1), w_r.at[m, k])

    def send_along_x(p):
        for dx in (2, 1, 3):
            send(
                rsx_s.at[dx, p], rsx_r.at[(-dx) % XN - 1, p],
                rx_s.at[dx - 1, p], rx_r.at[(-dx) % XN - 1, p], zx(0, dx), t,
            )

    def mixer(group):
        blocks = [(dx, ZPOS[dz]) for dx in range(XN) for dz in group]
        count = SUB * len(blocks)
        for dz in group:
            p = ZPOS[dz]
            if dz in NEXT:
                await_bytes(xbuf.at[:, p], gz_r.at[p - 1])
            elif dz in DIRECT_IN:
                if dz != 0:
                    for dx in range(XN):
                        await_bytes(xbuf.at[dx, p], az_r.at[dx, p])
            else:
                for dx in range(1, XN):
                    await_bytes(xbuf.at[dx, p], xf_r.at[dx - 1, p])
        for i, (dx, p) in enumerate(blocks):
            block = xbuf[dx, p].astype(F32)
            for j in range(TN):
                xs[SUB * i : SUB * (i + 1), DB * j : DB * (j + 1)] = block[j]
        sec = xs[:count, :]
        scale_two = lax.rsqrt(jnp.sum(sec * sec, axis=-1, keepdims=True) * (1.0 / D) + EPS)
        scaled = (sec * gains[...]).astype(BF16)
        preact = jnp.dot(scaled, upb[...], preferred_element_type=F32)
        hidden = jnp.square(jnp.maximum(preact * scale_two, 0.0)).astype(BF16)
        for j in range(TN):
            os[:count, DB * j : DB * (j + 1)] = jnp.dot(hidden, dnb[j], preferred_element_type=F32)
        for i, (dx, p) in enumerate(blocks):
            for j in range(TN):
                block = os[SUB * i : SUB * (i + 1), DB * j : DB * (j + 1)]
                if p == HOME:
                    own_row[dx, j] = block
                elif dx == 0 and ZORD[p] not in DIRECT_OUT + NEXT:
                    own[p, j] = block
                else:
                    rsx_s[dx, p, j] = block.astype(BF16)
        for dz in group:
            p = ZPOS[dz]
            if dz in DIRECT_OUT:
                for dx in (2, 1, 3, 0):
                    scatter(dz, dx, rsx_s.at[dx, p], fin, fi_s, fi_r)
            elif dz in NEXT:
                there = ZPOS[(-dz) % ZN] - 1
                send(rsx_s.at[:, p], rows_z.at[there], hz_s.at[p - 1], hz_r.at[there], zx(dz, 0), t)
            elif dz != 0:
                send_along_x(p)

    def sum_z():
        for k in range(2):
            await_bytes(rows_z.at[k], hz_r.at[k])
        for dx in range(XN):
            total = own_row[dx] + rows_z[0, dx].astype(F32) + rows_z[1, dx].astype(F32)
            if dx == 0:
                own[HOME] = total
            else:
                rsx_s[dx, HOME] = total.astype(BF16)
        send_along_x(HOME)

    def sum_x(p):
        for dx in range(1, XN):
            await_bytes(rsx_r.at[dx - 1, p], rx_r.at[dx - 1, p])
        total = own[p]
        for dx in range(1, XN):
            total += rsx_r[dx - 1, p].astype(F32)
        zs[p] = total.astype(BF16)
        scatter(ZORD[p], 0, zs.at[p], fin, fi_s, fi_r)

    for step in ORDER:
        group = [int(digit) for digit in step[1:]]
        if step == "w":
            rest_of_weights()
        elif step == "d":
            spread_row()
        elif step == "z":
            sum_z()
        elif step[0] == "r":
            relay(group[0], 2, 2, None)
        elif step[0] == "f":
            forward(group[0])
        elif step[0] == "m":
            mixer(group)
        else:
            sum_x(ZPOS[group[0]])

    for src, sem in pending:
        await_bytes(src, sem)
    for p in range(ZN):
        for dx in targets(ZORD[p], DIRECT_IN):
            count = TN - 1 if ZORD[p] == 0 and dx == 0 else TN
            await_bytes(seg.at[pl.ds(0, count)], az_s.at[dx, p])

    total = jnp.zeros((TN, SUB, DB), F32)
    for p in range(ZN):
        for dx in targets(ZORD[p], DIRECT_OUT):
            await_bytes(fin.at[dx, p], fi_r.at[dx, p])
            total += fin[dx, p].astype(F32)
    for s in range(TN):
        of[SUB * s : SUB * (s + 1), :] = total[s]
    out_ref[...] = (secf[...] + of[...]).astype(BF16)

    for p in range(ZN):
        for dx in targets(ZORD[p], DIRECT_OUT):
            count = TN - 1 if ZORD[p] == 0 and dx == 0 else TN
            await_bytes(seg.at[pl.ds(0, count)], fi_s.at[dx, p])
    store_mem.wait()


def write_out(*refs):
    ins, outs, sems = refs[:4], refs[4:8], refs[8]
    copies = [pltpu.make_async_copy(ins[k], outs[k], sems.at[k]) for k in (1, 0, 2, 3)]
    for copy in copies:
        copy.start()
    for copy in copies:
        copy.wait()


def per_device(
    tokens, memory, normalizer, stabilizer, norm_gain, query_weight, key_weight, value_weight, outgate_weight,
    input_gate_weight, forget_gate_weight, forget_bias, memory_gain, proj_weight, ffn_gain, up_weight, down_weight,
):
    hbm = pl.BlockSpec(memory_space=pltpu.HBM)
    anywhere = pl.BlockSpec(memory_space=pl.ANY)
    vmem = pl.BlockSpec(memory_space=pltpu.VMEM)
    dma = pltpu.SemaphoreType.DMA
    outs = (
        jax.ShapeDtypeStruct((ROWS, DB), BF16),
        jax.ShapeDtypeStruct((ROWS, DK, DK), F32),
        jax.ShapeDtypeStruct((ROWS, DK), F32),
        jax.ShapeDtypeStruct((1, ROWS), F32),
    )
    layer_out, memory_new, normalizer_new, stab_new = pl.pallas_call(
        kernel,
        out_shape=outs,
        in_specs=[hbm] * 17,
        out_specs=(vmem, anywhere, vmem, vmem),
        scratch_shapes=[
            pltpu.VMEM((ROWS, D), BF16),
            pltpu.VMEM((ROWS, DK, DK), F32),
            pltpu.VMEM((ROWS, DK), F32),
            pltpu.VMEM((1, ROWS), F32),
            pltpu.VMEM((1, D), F32),
            pltpu.VMEM((D, 4 * DK), BF16),
            pltpu.VMEM((TN, D), BF16),
            pltpu.VMEM((TN, D), BF16),
            pltpu.VMEM((1, TN), F32),
            pltpu.VMEM((1, DK), F32),
            pltpu.VMEM((TN * DK, DB), BF16),
            pltpu.VMEM((1, D), F32),
            pltpu.VMEM((D, FB), BF16),
            pltpu.VMEM((TN, FB, DB), BF16),
            pltpu.VMEM((ROWS, DK), F32),
            pltpu.VMEM((2, ROWS, DK), F32),
            pltpu.VMEM((DK, DK), F32),
            pltpu.VMEM((ROWS, TN * DK), BF16),
            pltpu.VMEM((ROWS, DB), F32),
            pltpu.VMEM((TN, SUB, DB), BF16),
            pltpu.VMEM((XN, ZN, TN, SUB, DB), BF16),
            pltpu.VMEM((ROWS, D), F32),
            pltpu.VMEM((ROWS, D), F32),
            pltpu.VMEM((XN, ZN, TN, SUB, DB), BF16),
            pltpu.VMEM((XN - 1, ZN, TN, SUB, DB), BF16),
            pltpu.VMEM((ZN, TN, SUB, DB), F32),
            pltpu.VMEM((XN, TN, SUB, DB), F32),
            pltpu.VMEM((2, XN, TN, SUB, DB), BF16),
            pltpu.VMEM((ZN, TN, SUB, DB), BF16),
            pltpu.VMEM((XN, ZN, TN, SUB, DB), BF16),
            pltpu.VMEM((ROWS, DB), F32),
            dma((18,)),
            dma((7,)), dma((7,)),
            dma((7,)), dma((7,)),
            dma((7,)), dma((7,)),
            dma((4, 7)), dma((4, 7)),
            dma((XN, ZN)), dma((XN, ZN)),
            dma((XN - 1, ZN)), dma((XN - 1, ZN)),
            dma((XN - 1, ZN)), dma((XN - 1, ZN)),
            dma((XN, ZN)), dma((XN, ZN)),
            dma((2,)), dma((2,)),
            dma((2,)), dma((2,)),
            pltpu.SemaphoreType.REGULAR((3,)),
            pltpu.SemaphoreType.REGULAR((2,)),
        ],
        compiler_params=pltpu.CompilerParams(
            collective_id=0, has_side_effects=True, vmem_limit_bytes=40 * 1024 * 1024
        ),
        name="layer",
    )(
        *(
            pltpu.with_memory_space_constraint(a, pltpu.HBM)
            for a in (
                tokens,
                memory.reshape(ROWS, DK, DK),
                normalizer.reshape(ROWS, DK),
                stabilizer.T,
                norm_gain.reshape(1, D),
                query_weight, key_weight, value_weight, outgate_weight,
                input_gate_weight.T,
                forget_gate_weight.T,
                forget_bias.reshape(1, TN),
                memory_gain.reshape(1, DK),
                proj_weight,
                ffn_gain.reshape(1, DB),
                up_weight,
                down_weight,
            )
        )
    )
    layer_out, memory_new, normalizer_new, stab_new = pl.pallas_call(
        write_out,
        out_shape=outs,
        in_specs=[anywhere] * 4,
        out_specs=(hbm,) * 4,
        scratch_shapes=[dma((4,))],
        compiler_params=pltpu.CompilerParams(vmem_limit_bytes=4 * 1024 * 1024),
        name="write_out",
    )(layer_out, memory_new, normalizer_new, stab_new)
    return (
        layer_out,
        memory_new.reshape(ROWS, 1, DK, DK),
        normalizer_new.reshape(ROWS, 1, DK),
        stab_new.T,
    )


def solution(mesh):
    placed = (
        P("kv", "tp"),
        P("kv", "tp", None, None),
        P("kv", "tp", None),
        P("kv", "tp"),
        P(),
        P(None, "tp"),
        P(None, "tp"),
        P(None, "tp"),
        P(None, "tp"),
        P(),
        P(),
        P(),
        P("tp"),
        P(None, "tp"),
        P("tp"),
        P("tp", "kv"),
        P("kv", "tp"),
    )
    outs = (P("kv", "tp"), P("kv", "tp", None, None), P("kv", "tp", None), P("kv", "tp"))
    return jax.shard_map(per_device, mesh=mesh, in_specs=placed, out_specs=outs, check_vma=False)
```
